32 devices in a mesh: ep: 32 (over z, y, x, core).
Axes of the slice: x: 2, y: 2, z: 4, core: 2. Of those that a mesh axis runs over, the one named last changes fastest.
Arguments:
- hidden_in: bfloat16 [512, 2048], P('ep'), may hold values from -6 to 6
- lengths: int32 [512], P('ep'), may hold values from 1 to 1024
- attn_gain: float32 [2048], replicated, may hold values from 0.1 to 1.9
- query_weight: bfloat16 [2048, 512], replicated, may hold values from -0.125 to 0.125
- key_weight: bfloat16 [2048, 128], replicated, may hold values from -0.125 to 0.125
- value_weight: bfloat16 [2048, 128], replicated, may hold values from -0.125 to 0.125
- score_bias: float32 [8], replicated, may hold values from -7.5 to -3.5
- out_weight: bfloat16 [512, 2048], replicated, may hold values from -0.25 to 0.25
- key_cache: bfloat16 [512, 1024, 128], P('ep'), may hold values from -6 to 6
- value_cache: bfloat16 [512, 1024, 128], P('ep'), may hold values from -10 to 10
- ffn_gain: float32 [2048], replicated, may hold values from 0.1 to 1.9
- routes: int32 [512, 4], P('ep'), may hold values from 0 to 31, all different within a row; in each aligned block of 16 rows (0 to 15, 16 to 31, ...) at most 2 rows name the same one
- route_weights: float32 [512, 4], P('ep'), may hold values from 0.25 to 1
- expert_gate: bfloat16 [32, 2048, 512], P('ep'), may hold values from -0.125 to 0.125
- expert_up: bfloat16 [32, 2048, 512], P('ep'), may hold values from -0.125 to 0.125
- expert_down: bfloat16 [32, 512, 2048], P('ep'), may hold values from -0.25 to 0.25
- dense_gate: bfloat16 [2048, 2048], P(None, 'ep'), may hold values from -0.125 to 0.125
- dense_up: bfloat16 [2048, 2048], P(None, 'ep'), may hold values from -0.125 to 0.125
- dense_down: bfloat16 [2048, 2048], P(None, 'ep'), may hold values from -0.125 to 0.125
- branch_gate: float32 [2048], replicated, may hold values from -0.125 to 0.125
Outputs:
- hidden_out: bfloat16 [512, 2048], P('ep')
- new_keys: bfloat16 [512, 128], P('ep')
- new_values: bfloat16 [512, 128], P('ep')
The draws below stay inside these ranges and needn't reach their ends.
Inputs may be any that keep to these rules, and one draw needn't show every extreme that they name: `routes`: in each device's 16 rows no expert is named twice.
All inputs are finite; a program needn't handle non-finite values.
Results may differ from the reference program's by a relative error of at most 0.0061.
Values may be sent and summed in bfloat16 or wider, within the bound.
No kernel may reach another device: no remote copies, remote signals or barrier semaphores. Data moves between devices by JAX's collectives and lax.ppermute only.
A program may use at most 128 MiB of HBM per device.

```python
import math
import jax
import jax.numpy as jnp
import numpy as np
from jax import lax

D = 2048
HEADS = 8
KV_HEADS = 2
HEAD = 64
LEN = 1024
EFF = 512
TOP = 4
FDENSE = 2048
SEQ_DEV = 16
CAP = 2
BATCH = 512
EXPERTS = 32


def draw_score_bias(key, part):
    base_key = jax.random.fold_in(key, 11)
    key_slow, key_fast, key_pick = jax.random.split(base_key, 3)
    slow_bias = jax.random.uniform(key_slow, (HEADS,), jnp.float32, -7.5, -6.5)
    fast_bias = jax.random.uniform(key_fast, (HEADS,), jnp.float32, -4.5, -3.5)
    head_order = jax.random.permutation(key_pick, HEADS)
    fast_heads = head_order < HEADS // 2
    return jnp.where(fast_heads, fast_bias, slow_bias)


def draw_value_cache(key, part):
    base_key = jax.random.fold_in(key, 23)
    key_noise, key_block, key_common = jax.random.split(base_key, 3)
    row_width = KV_HEADS * HEAD
    noise_part = jax.random.normal(key_noise, (BATCH, LEN, row_width), jnp.float32)
    block_means = jax.random.normal(key_block, (BATCH, 8, row_width), jnp.float32)
    span_means = jnp.repeat(block_means, LEN // 8, axis=1)
    values_out = noise_part + span_means
    return jnp.clip(values_out, -10.0, 10.0).astype(jnp.bfloat16)


def place_ends(values, key, smallest, high):
    extent = values.shape
    place = [jax.random.randint(jax.random.fold_in(key, axis), (), 0, extent[axis]) for axis in range(len(extent))]
    values = values.at[tuple(place)].set(smallest)
    longest = extent.index(max(extent))
    place[longest] = (place[longest] + 1) % extent[longest]
    return values.at[tuple(place)].set(high)


def block_scale(stream_key, extent, cuts, smallest, largest):
    loudness = 1.0
    for position, blocks in cuts:
        steps = jax.random.uniform(jax.random.fold_in(jax.random.fold_in(stream_key, 6), position), (blocks,), jnp.float32, smallest / len(cuts), largest / len(cuts))
        loudness = loudness * jnp.repeat(jnp.exp(steps), extent[position] // blocks).reshape((-1,) + (1,) * (len(extent) - 1 - position))
    return loudness


def deal_out(key, own, number, rows, number_of, top, most, slope):
    sequence = jax.random.permutation(key, number_of)
    heavy_load, common = shares(number_of, rows * top, most, slope, True), shares(number_of, rows * top, most, slope, False)
    places = jnp.arange(number_of)

    def named(sizes, turn):
        used = int((sizes > 0).sum())
        fixed = max(1, used // 4)
        moved = fixed + (places - fixed + turn * (used - fixed)) % max(1, number_of - fixed)
        return jnp.zeros((number_of,), jnp.int32).at[sequence[jnp.where(places < fixed, places, moved)]].set(jnp.asarray(sizes, jnp.int32))

    sizes = jnp.where(number % 4 == 0, named(heavy_load, number // 4), named(common, number - number // 4 - 1))
    mixed = jax.random.permutation(jax.random.fold_in(own, 3), number_of)
    giver, receiver = mixed[0:number_of // 2 * 2:2], mixed[1:number_of // 2 * 2:2]
    slack = jnp.minimum(sizes[giver] - 1, most - sizes[receiver]) // 2
    slack = jnp.where((giver == sequence[0]) | (receiver == sequence[0]) | (sizes[receiver] == 0), 0, jnp.maximum(slack, 0))
    moved = jax.random.randint(jax.random.fold_in(own, 4), (number_of // 2,), 0, 1 << 20) % (slack + 1)
    sizes = sizes.at[giver].add(-moved).at[receiver].add(moved)
    items = jnp.searchsorted(jnp.cumsum(sizes), jnp.arange(rows * top), side="right").astype(jnp.int32)
    grid = items.reshape(top, rows).T
    grid = grid[jax.random.permutation(jax.random.fold_in(own, 1), rows)]
    turn = jax.random.randint(jax.random.fold_in(own, 2), (rows, 1), 0, top)
    return jnp.take_along_axis(grid, (jnp.arange(top)[None, :] + turn) % top, axis=1)


def shares(count, total, most, skew, full):
    weights = [(1 << 20) // math.isqrt(grade ** skew) + 1 for grade in range(1, count + 1)]
    largest = most if full else min(most, max(-(-total // count), total * weights[0] // sum(weights)))
    least = 1 if total - largest >= count - 1 else 0
    counts, rest = [largest] + [least] * (count - 1), total - largest - least * (count - 1)
    while rest > 0:
        candidates = [i for i in range(1, count) if counts[i] < largest] or [i for i in range(1, count) if counts[i] < most]
        whole, left = sum([weights[i] for i in candidates]), rest
        for i in candidates:
            extra = min(most - counts[i], max(1, left * weights[i] // whole), rest)
            counts[i] = counts[i] + extra
            rest = rest - extra
    return np.array(counts)


def normal_values(own_key, extent, spread, most, cuts=(), kind=jnp.bfloat16):
    drawn = jax.random.normal(own_key, extent, jnp.float32) * spread
    if len(cuts) > 0:
        drawn = block_scale(own_key, extent, cuts, -0.22, 0.18) * drawn
    return jnp.clip(drawn, min=-most, max=most).astype(kind)


def setup_inputs(seed: int = 0) -> dict:
    seeds = jax.random.split(jax.random.key(seed), 21)
    hidden_in = normal_values(seeds[0], (BATCH, D), 1.0, 6.0, ((0, 32),))
    lengths = place_ends(jax.random.randint(seeds[1], (BATCH,), 1, LEN + 1), jax.random.fold_in(seeds[1], 1), 1, LEN).astype(jnp.int32)
    attn_gain = jnp.clip(1.0 + 0.18 * jax.random.normal(seeds[2], (D,), jnp.float32), 0.1, 1.9)
    query_weight = normal_values(seeds[3], (D, HEADS * HEAD), D ** -0.5, 0.125)
    key_weight = normal_values(seeds[4], (D, KV_HEADS * HEAD), D ** -0.5, 0.125)
    value_weight = normal_values(seeds[5], (D, KV_HEADS * HEAD), D ** -0.5, 0.125)
    score_bias = draw_score_bias(jax.random.fold_in(seeds[20], 71), 0)
    out_weight = normal_values(seeds[7], (HEADS * HEAD, D), (HEADS * HEAD) ** -0.5, 0.25)
    key_cache = normal_values(seeds[8], (BATCH, LEN, KV_HEADS * HEAD), 1.0, 6.0, ((0, 32),))
    value_cache = draw_value_cache(jax.random.fold_in(seeds[20], 71), 0)
    ffn_gain = jnp.clip(1.0 + 0.18 * jax.random.normal(seeds[10], (D,), jnp.float32), 0.1, 1.9)
    routes_keys = jax.random.split(jax.random.fold_in(seeds[11], 1), BATCH // SEQ_DEV)
    routes_turns = jax.random.permutation(jax.random.fold_in(seeds[11], 3), BATCH // SEQ_DEV)
    routes = jax.vmap(lambda own, number: deal_out(jax.random.fold_in(seeds[11], 2), own, number, SEQ_DEV, EXPERTS, TOP, CAP, 2))(routes_keys, routes_turns).reshape((BATCH, TOP))
    route_weights = jnp.clip(0.25 + 0.75 * jax.random.uniform(seeds[12], (BATCH, TOP), jnp.float32) ** block_scale(seeds[12], (BATCH, TOP), ((0, 32),), -0.2, 0.2), 0.25, 1.0)
    expert_gate = normal_values(seeds[13], (EXPERTS, D, EFF), D ** -0.5, 0.125, ((0, 32),))
    expert_up = normal_values(seeds[14], (EXPERTS, D, EFF), D ** -0.5, 0.125, ((0, 32),))
    expert_down = normal_values(seeds[15], (EXPERTS, EFF, D), EFF ** -0.5, 0.25, ((0, 32),))
    dense_gate = normal_values(seeds[16], (D, FDENSE), D ** -0.5, 0.125, ((1, 32),))
    dense_up = normal_values(seeds[17], (D, FDENSE), D ** -0.5, 0.125, ((1, 32),))
    dense_down = normal_values(seeds[18], (D, FDENSE), FDENSE ** -0.5, 0.125, ((1, 32),))
    branch_gate = normal_values(seeds[19], (D,), D ** -0.5, 0.125, (), jnp.float32)
    return dict(hidden_in=hidden_in, lengths=lengths, attn_gain=attn_gain, query_weight=query_weight, key_weight=key_weight, value_weight=value_weight, score_bias=score_bias, out_weight=out_weight, key_cache=key_cache, value_cache=value_cache, ffn_gain=ffn_gain, routes=routes, route_weights=route_weights, expert_gate=expert_gate, expert_up=expert_up, expert_down=expert_down, dense_gate=dense_gate, dense_up=dense_up, dense_down=dense_down, branch_gate=branch_gate)


norm_eps = 1e-06

def rms_norm(values_in, gain):
    as_float = values_in.astype(jnp.float32)
    scaled = as_float * lax.rsqrt(lax.optimization_barrier(jnp.mean(as_float * as_float, axis=-1, keepdims=True)) + norm_eps)
    return (scaled * gain).astype(jnp.bfloat16)

def stick_attend(query_blk, key_blk, value_blk, seq_lens, score_bias):
    seq_count = query_blk.shape[0]
    per_group = HEADS // KV_HEADS
    query_f = query_blk.astype(jnp.float32).reshape(seq_count, KV_HEADS, per_group, HEAD)
    key_f = key_blk.astype(jnp.float32).reshape(seq_count, LEN, KV_HEADS, HEAD)
    value_f = value_blk.astype(jnp.float32).reshape(seq_count, LEN, KV_HEADS, HEAD)
    head_bias = score_bias.astype(jnp.float32).reshape(KV_HEADS, per_group)[None, :, :, None]
    scores = jnp.einsum('nkgd,nskd->nkgs', query_f, key_f) * HEAD ** (-0.5) + head_bias
    live_mask = (jnp.arange(LEN, dtype=jnp.int32)[None, :] < seq_lens[:, None])[:, None, None, :]
    log_keep = jnp.where(live_mask, jax.nn.log_sigmoid(-scores), 0.0)
    after_sum = lax.cumsum(log_keep, axis=3, reverse=True) - log_keep
    weights = jnp.where(live_mask, jnp.exp(jax.nn.log_sigmoid(scores) + after_sum), 0.0).astype(jnp.bfloat16)
    weights = lax.optimization_barrier(weights)
    mixed = jnp.einsum('nkgs,nskd->nkgd', weights.astype(jnp.float32), value_f)
    return mixed.astype(jnp.bfloat16).reshape(seq_count, HEADS * HEAD)

def reference(hidden_in, lengths, attn_gain, query_weight, key_weight, value_weight, score_bias, out_weight, key_cache, value_cache, ffn_gain, routes, route_weights, expert_gate, expert_up, expert_down, dense_gate, dense_up, dense_down, branch_gate):
    normed = rms_norm(hidden_in, attn_gain)
    queries = jnp.dot(normed, query_weight, preferred_element_type=jnp.float32).astype(jnp.bfloat16)
    new_keys = jnp.dot(normed, key_weight, preferred_element_type=jnp.float32).astype(jnp.bfloat16)
    new_values = jnp.dot(normed, value_weight, preferred_element_type=jnp.float32).astype(jnp.bfloat16)
    blocks = BATCH // SEQ_DEV

    def attend_block(pieces):
        return stick_attend(pieces[0], pieces[1], pieces[2], pieces[3], score_bias)
    attended = lax.map(attend_block, (queries.reshape(blocks, SEQ_DEV, HEADS * HEAD), key_cache.reshape(blocks, SEQ_DEV, LEN, KV_HEADS * HEAD), value_cache.reshape(blocks, SEQ_DEV, LEN, KV_HEADS * HEAD), lengths.reshape(blocks, SEQ_DEV)))
    attended = attended.reshape(BATCH, HEADS * HEAD)
    middle = hidden_in.astype(jnp.float32) + jnp.dot(attended, out_weight, preferred_element_type=jnp.float32)
    ffn_in = rms_norm(middle, ffn_gain)

    def one_token(pieces):
        token_row, expert_ids, pick_weights = pieces
        row_f = token_row.astype(jnp.float32)
        gate_pre = jnp.einsum('d,kdf->kf', row_f, expert_gate[expert_ids].astype(jnp.float32))
        up_pre = jnp.einsum('d,kdf->kf', row_f, expert_up[expert_ids].astype(jnp.float32))
        hidden_act = lax.optimization_barrier((jax.nn.silu(gate_pre) * up_pre).astype(jnp.bfloat16))
        expert_rows = jnp.einsum('kf,kfd->kd', hidden_act.astype(jnp.float32), expert_down[expert_ids].astype(jnp.float32)).astype(jnp.bfloat16)
        expert_rows = lax.optimization_barrier(expert_rows)
        return lax.optimization_barrier(jnp.sum(pick_weights[:, None] * expert_rows.astype(jnp.float32), axis=0))
    expert_sum = lax.map(one_token, (ffn_in, routes, route_weights))
    gate_pre = jnp.dot(ffn_in, dense_gate, preferred_element_type=jnp.float32)
    up_pre = jnp.dot(ffn_in, dense_up, preferred_element_type=jnp.float32)
    dense_hidden = (jax.nn.silu(gate_pre) * up_pre).astype(jnp.bfloat16)
    dense_out = jnp.dot(dense_hidden, dense_down.T, preferred_element_type=jnp.float32)
    gate_value = jax.nn.sigmoid(jnp.dot(ffn_in.astype(jnp.float32), branch_gate, precision=lax.Precision.HIGHEST))
    hidden_out = (middle + expert_sum + gate_value[:, None] * dense_out).astype(jnp.bfloat16)
    return (hidden_out, new_keys, new_values)
```

```python
import jax
import jax.numpy as jnp
from jax import lax
from jax.experimental import pallas as pl
from jax.experimental.pallas import tpu as pltpu
from jax.sharding import PartitionSpec as P

HEADS = 8
KV_HEADS = 2
HEAD = 64
TOP = 4
GROUP = HEADS // KV_HEADS
KV_WIDTH = KV_HEADS * HEAD
CHUNK = 256

norm_eps = 1e-06
bf16 = jnp.bfloat16
f32 = jnp.float32


def iota(shape, dim):
    return lax.broadcasted_iota(jnp.int32, shape, dim)


def matmul(left, right):
    return jnp.dot(left, right, preferred_element_type=f32)


def matmul_bt(left, right):
    return lax.dot_general(left, right, (((1,), (1,)), ((), ())), preferred_element_type=f32)


def matmul_at(left, right):
    return lax.dot_general(left, right, (((0,), (0,)), ((), ())), preferred_element_type=f32)


def rms_rows(values, gain):
    scale = lax.rsqrt(jnp.mean(values * values, axis=-1, keepdims=True) + norm_eps)
    return (values * scale * gain).astype(bf16)


def three_parts(values):
    high = values.astype(bf16)
    rest = values - high.astype(f32)
    middle = rest.astype(bf16)
    low = (rest - middle.astype(f32)).astype(bf16)
    return high, middle, low


def attend_kernel(
    capacity,
    lengths,
    score_bias,
    hidden,
    attn_gain,
    ffn_gain,
    branch_gate,
    routes_t,
    route_weights_t,
    query_hbm,
    key_hbm,
    value_hbm,
    keys_hbm,
    values_hbm,
    out_hbm,
    new_keys,
    new_values,
    middle,
    ffn_in,
    outgoing,
    combine,
    gate_value,
    query_w,
    key_w,
    value_w,
    keys,
    values,
    out_w,
    blocked,
    weights_t,
    weight_sems,
    key_sems,
    value_sems,
    out_sem,
):
    seqs = hidden.shape[0]
    cache_len = keys.shape[1]
    lanes = seqs * HEADS
    chunks = cache_len // CHUNK
    pairs = seqs // 2

    first = [
        pltpu.make_async_copy(query_hbm, query_w, weight_sems.at[0]),
        pltpu.make_async_copy(key_hbm, key_w, weight_sems.at[1]),
        pltpu.make_async_copy(value_hbm, value_w, weight_sems.at[2]),
    ]
    key_copies = [
        pltpu.make_async_copy(
            keys_hbm.at[:, pl.ds(c * CHUNK, CHUNK), :],
            keys.at[:, pl.ds(c * CHUNK, CHUNK), :],
            key_sems.at[c],
        )
        for c in range(chunks)
    ]
    value_copies = [
        pltpu.make_async_copy(
            values_hbm.at[pl.ds(p * 2, 2)], values.at[pl.ds(p * 2, 2)], value_sems.at[p]
        )
        for p in range(pairs)
    ]
    out_copy = pltpu.make_async_copy(out_hbm, out_w, out_sem)
    for copy in first:
        copy.start()
    for copy in reversed(key_copies):
        copy.start()
    for copy in value_copies:
        copy.start()
    out_copy.start()

    hidden_f = hidden[...].astype(f32)
    normed = rms_rows(hidden_f, attn_gain[...])

    lane = iota((1, lanes), 1)
    lane_len = jnp.zeros((1, lanes), jnp.int32)
    for n in range(seqs):
        lane_len = jnp.where(lane // HEADS == n, lengths[n], lane_len)
    lane_bias = jnp.zeros((1, lanes), f32)
    for h in range(HEADS):
        lane_bias = jnp.where(lane % HEADS == h, score_bias[h], lane_bias)

    spread = (iota((lanes, seqs), 0) // HEADS == iota((lanes, seqs), 1)).astype(bf16)
    gather = (iota((seqs, lanes), 1) // HEADS == iota((seqs, lanes), 0)).astype(bf16)
    wide = (lanes, HEADS * HEAD)
    own_head = iota(wide, 1) // HEAD == iota(wide, 0) % HEADS
    fold_shape = (HEADS * HEAD, KV_WIDTH)
    fold = (
        (iota(fold_shape, 0) // (HEAD * GROUP) == iota(fold_shape, 1) // HEAD)
        & (iota(fold_shape, 0) % HEAD == iota(fold_shape, 1) % HEAD)
    ).astype(bf16)
    later = (iota((CHUNK, CHUNK), 1) > iota((CHUNK, CHUNK), 0)).astype(bf16)

    for copy in first:
        copy.wait()
    queries = matmul(normed, query_w[...]).astype(bf16)
    new_keys[...] = matmul(normed, key_w[...]).astype(bf16)
    new_values[...] = matmul(normed, value_w[...]).astype(bf16)

    spread_q = jnp.where(own_head, matmul(spread, queries), 0.0).astype(bf16)
    by_head = jnp.transpose(matmul(spread_q, fold))
    square = (KV_WIDTH, lanes)
    for n in range(seqs):
        own_lane = iota(square, 1) // HEADS == n
        blocked[n * KV_WIDTH : (n + 1) * KV_WIDTH, :] = jnp.where(own_lane, by_head, 0.0).astype(
            bf16
        )

    carry = jnp.zeros((1, lanes), f32)
    for c in reversed(range(chunks)):
        key_copies[c].wait()
        rows = slice(c * CHUNK, (c + 1) * CHUNK)
        key_rows = jnp.concatenate([keys[n, rows, :] for n in range(seqs)], axis=1)
        scores = matmul(key_rows, blocked[...]) * HEAD ** (-0.5) + lane_bias
        live = iota((CHUNK, lanes), 0) + c * CHUNK < lane_len
        soft = jnp.log1p(jnp.exp(-jnp.abs(scores)))
        log_keep = jnp.where(live, jnp.minimum(-scores, 0.0) - soft, 0.0)
        log_take = jnp.minimum(scores, 0.0) - soft
        sums = matmul(later, jnp.concatenate(three_parts(log_keep), axis=1))
        after = sums[:, :lanes] + sums[:, lanes : 2 * lanes] + sums[:, 2 * lanes :] + carry
        carry = carry + jnp.sum(log_keep, axis=0, keepdims=True)
        taken = jnp.where(live, jnp.exp(log_take + after), 0.0)
        weights_t[:, rows] = jnp.transpose(taken).astype(bf16)

    pieces = []
    for p in range(pairs):
        value_copies[p].wait()
        value_rows = jnp.concatenate([values[2 * p], values[2 * p + 1]], axis=1)
        mixed = matmul(weights_t[2 * p * HEADS : 2 * (p + 1) * HEADS, :], value_rows)
        pieces.append(mixed[:HEADS, :KV_WIDTH])
        pieces.append(mixed[HEADS:, KV_WIDTH:])
    mixed = jnp.concatenate(pieces, axis=0)
    own_group = (iota(mixed.shape, 0) % HEADS) // GROUP == iota(mixed.shape, 1) // HEAD
    mixed = jnp.where(own_group, mixed, 0.0).astype(bf16)
    unfolded = jnp.where(own_head, matmul_bt(mixed, fold), 0.0).astype(bf16)
    attended = matmul(gather, unfolded).astype(bf16)

    out_copy.wait()
    middle_f = hidden_f + matmul(attended, out_w[...])
    middle[...] = middle_f
    ffn = rms_rows(middle_f, ffn_gain[...])
    ffn_in[...] = ffn
    gate_sum = jnp.sum(ffn.astype(f32) * branch_gate[...], axis=-1, keepdims=True)
    gate_value[...] = jnp.broadcast_to(jax.nn.sigmoid(gate_sum), gate_value.shape)

    slots = (outgoing.shape[0], seqs)
    expert = iota(slots, 0) // capacity
    named = jnp.zeros(slots, f32)
    weighted = jnp.zeros(slots, f32)
    for k in range(TOP):
        hit = expert == routes_t[k : k + 1, :]
        named = named + jnp.where(hit, 1.0, 0.0)
        weighted = weighted + jnp.where(hit, route_weights_t[k : k + 1, :], 0.0)
    earlier = (iota((seqs, seqs), 0) < iota((seqs, seqs), 1)).astype(bf16)
    rank = matmul(named.astype(bf16), earlier)
    mine = rank == (iota(slots, 0) % capacity).astype(f32)
    combine[...] = jnp.where(mine, weighted, 0.0)
    outgoing[...] = matmul(jnp.where(mine, named, 0.0).astype(bf16), ffn).astype(bf16)


def attend(capacity, slots, args):
    hidden = args[2]
    keys = args[11]
    seqs, width = hidden.shape
    cache_len = keys.shape[1]
    pairs = seqs // 2
    shapes = (
        jax.ShapeDtypeStruct((seqs, KV_WIDTH), bf16),
        jax.ShapeDtypeStruct((seqs, KV_WIDTH), bf16),
        jax.ShapeDtypeStruct((seqs, width), f32),
        jax.ShapeDtypeStruct((seqs, width), bf16),
        jax.ShapeDtypeStruct((slots, width), bf16),
        jax.ShapeDtypeStruct((slots, seqs), f32),
        jax.ShapeDtypeStruct((seqs, 128), f32),
    )
    smem = pl.BlockSpec(memory_space=pltpu.SMEM)
    vmem = pl.BlockSpec(memory_space=pltpu.VMEM)
    hbm = pl.BlockSpec(memory_space=pl.ANY)
    big = args[8:]
    return pl.pallas_call(
        lambda *refs: attend_kernel(capacity, *refs),
        out_shape=shapes,
        in_specs=[smem] * 2 + [vmem] * 6 + [hbm] * 6,
        out_specs=[vmem] * 7,
        scratch_shapes=[pltpu.VMEM(a.shape, a.dtype) for a in big]
        + [
            pltpu.VMEM((seqs * KV_WIDTH, seqs * HEADS), bf16),
            pltpu.VMEM((seqs * HEADS, cache_len), bf16),
            pltpu.SemaphoreType.DMA((3,)),
            pltpu.SemaphoreType.DMA((cache_len // CHUNK,)),
            pltpu.SemaphoreType.DMA((pairs,)),
            pltpu.SemaphoreType.DMA,
        ],
        compiler_params=pltpu.CompilerParams(vmem_limit_bytes=40 << 20),
        name="attend",
    )(*args)


def per_device(
    hidden_in,
    lengths,
    attn_gain,
    query_weight,
    key_weight,
    value_weight,
    score_bias,
    out_weight,
    key_cache,
    value_cache,
    ffn_gain,
    routes,
    route_weights,
    expert_gate,
    expert_up,
    expert_down,
    dense_gate,
    dense_up,
    dense_down,
    branch_gate,
):
    seqs, width = hidden_in.shape
    devices = lax.axis_size("ep")
    local_experts = expert_gate.shape[0]
    experts_all = local_experts * devices
    capacity = max(1, seqs * TOP // experts_all)
    slots = experts_all * capacity
    layers = 1
    while 2 * (2 * layers) ** 2 <= devices and devices % (4 * layers) == 0:
        layers = 2 * layers
    plane = devices // layers
    units = dense_gate.shape[1]

    def swap(values, bits):
        return lax.ppermute(values, "ep", [(i, i ^ bits) for i in range(devices)])

    def climb(values, steps):
        return lax.ppermute(
            values, "ep", [(i, (i + steps * plane) % devices) for i in range(devices)]
        )

    own_dense = jnp.concatenate([dense_gate.T, dense_up.T, dense_down.T], axis=0)
    dense_parts = [own_dense]
    for other in range(2, plane, 2):
        dense_parts.append(swap(own_dense, other))

    new_keys, new_values, middle, ffn_in, outgoing, combine, gate_value = attend(
        capacity,
        slots,
        (
            lengths,
            score_bias,
            hidden_in,
            attn_gain.reshape(1, width),
            ffn_gain.reshape(1, width),
            branch_gate.reshape(1, width),
            routes.T,
            route_weights.T,
            query_weight,
            key_weight,
            value_weight,
            key_cache,
            value_cache,
            out_weight,
        ),
    )

    outgoing = outgoing.reshape(devices, local_experts * capacity, width)
    arrived = lax.all_to_all(outgoing, "ep", split_axis=0, concat_axis=0, tiled=True)
    chain = [ffn_in] + [climb(ffn_in, k) for k in range(1, layers)]
    chain = jnp.concatenate(chain, axis=0)
    chain = jnp.concatenate([chain, swap(chain, 1)], axis=0)

    flat_in = arrived.reshape(-1, width)
    gate_pre = matmul(flat_in, expert_gate[0])
    up_pre = matmul(flat_in, expert_up[0])
    hidden_act = (jax.nn.silu(gate_pre) * up_pre).astype(bf16)
    expert_rows = matmul(hidden_act, expert_down[0]).astype(bf16)
    returned = lax.all_to_all(
        expert_rows.reshape(arrived.shape), "ep", split_axis=0, concat_axis=0, tiled=True
    ).reshape(slots, width)

    gates = jnp.concatenate([part[:units] for part in dense_parts], axis=0)
    ups = jnp.concatenate([part[units : 2 * units] for part in dense_parts], axis=0)
    downs = jnp.concatenate([part[2 * units :] for part in dense_parts], axis=0)
    dense_hidden = (
        jax.nn.silu(matmul_bt(chain, gates)) * matmul_bt(chain, ups)
    ).astype(bf16)
    partial = matmul(dense_hidden, downs)
    half = layers * seqs
    summed = partial[:half] + swap(partial[half:].astype(bf16), 1).astype(f32)
    dense_out = summed[:seqs]
    for k in range(1, layers):
        piece = summed[k * seqs : (k + 1) * seqs].astype(bf16)
        dense_out = dense_out + climb(piece, -k).astype(f32)

    expert_sum = lax.dot_general(
        combine,
        returned.astype(f32),
        (((0,), (0,)), ((), ())),
        precision=lax.Precision.HIGHEST,
        preferred_element_type=f32,
    )
    hidden_out = (middle + expert_sum + gate_value[:, :1] * dense_out).astype(bf16)
    return (hidden_out, new_keys, new_values)


def solution(mesh):
    return jax.shard_map(
        per_device,
        mesh=mesh,
        in_specs=(
            P("ep", None),
            P("ep"),
            P(),
            P(),
            P(),
            P(),
            P(),
            P(),
            P("ep", None, None),
            P("ep", None, None),
            P(),
            P("ep", None),
            P("ep", None),
            P("ep", None, None),
            P("ep", None, None),
            P("ep", None, None),
            P(None, "ep"),
            P(None, "ep"),
            P(None, "ep"),
            P(),
        ),
        out_specs=(P("ep", None), P("ep", None), P("ep", None)),
        check_vma=False,
    )
```

```python
import jax
import jax.numpy as jnp
from jax import lax
from jax.experimental import pallas as pl
from jax.experimental.pallas import tpu as pltpu
from jax.sharding import PartitionSpec as P

HEADS = 8
KV_HEADS = 2
HEAD = 64
TOP = 4
GROUP = HEADS // KV_HEADS
KV_WIDTH = KV_HEADS * HEAD
CHUNK = 256


norm_eps = 1e-06
bf16 = jnp.bfloat16
f32 = jnp.float32


def iota(shape, dim):
    return lax.broadcasted_iota(jnp.int32, shape, dim)


def matmul(left, right):
    return jnp.dot(left, right, preferred_element_type=f32)


def matmul_bt(left, right):
    return lax.dot_general(left, right, (((1,), (1,)), ((), ())), preferred_element_type=f32)


def matmul_at(left, right):
    return lax.dot_general(left, right, (((0,), (0,)), ((), ())), preferred_element_type=f32)


def rms_rows(values, gain):
    scale = lax.rsqrt(jnp.mean(values * values, axis=-1, keepdims=True) + norm_eps)
    return (values * scale * gain).astype(bf16)


def three_parts(values):
    high = values.astype(bf16)
    rest = values - high.astype(f32)
    middle = rest.astype(bf16)
    low = (rest - middle.astype(f32)).astype(bf16)
    return high, middle, low


def attend_kernel(
    lengths_hbm,
    bias_hbm,
    hidden_hbm,
    attn_gain_hbm,
    ffn_gain_hbm,
    branch_hbm,
    dispatch,
    query_hbm,
    key_hbm,
    value_hbm,
    keys_hbm,
    values_hbm,
    out_hbm,
    expert_gate_hbm,
    new_keys,
    new_values,
    middle_hbm,
    ffn_hbm,
    outgoing_hbm,
    gate_value,
    expert_gate,
    lengths,
    score_bias,
    hidden,
    attn_gain,
    ffn_gain,
    branch_gate,
    query_w,
    key_w,
    value_w,
    keys,
    values,
    out_w,
    middle,
    ffn_in,
    outgoing,
    blocked,
    weights_t,
    small_sems,
    weight_sems,
    key_sems,
    value_sems,
    out_sem,
    expert_sem,
    send_sems,
):
    seqs = hidden.shape[0]
    cache_len = keys.shape[1]
    lanes = seqs * HEADS
    chunks = cache_len // CHUNK
    pairs = seqs // 2

    small = [
        pltpu.make_async_copy(source, target, small_sems.at[i])
        for i, (source, target) in enumerate(
            (
                (hidden_hbm, hidden),
                (attn_gain_hbm, attn_gain),
                (lengths_hbm, lengths),
                (bias_hbm, score_bias),
                (ffn_gain_hbm, ffn_gain),
                (branch_hbm, branch_gate),
            )
        )
    ]
    expert_copy = pltpu.make_async_copy(expert_gate_hbm, expert_gate, expert_sem)
    first = [
        pltpu.make_async_copy(query_hbm, query_w, weight_sems.at[0]),
        pltpu.make_async_copy(key_hbm, key_w, weight_sems.at[1]),
        pltpu.make_async_copy(value_hbm, value_w, weight_sems.at[2]),
    ]
    key_copies = [
        pltpu.make_async_copy(
            keys_hbm.at[:, pl.ds(c * CHUNK, CHUNK), :],
            keys.at[:, pl.ds(c * CHUNK, CHUNK), :],
            key_sems.at[c],
        )
        for c in range(chunks)
    ]
    value_copies = [
        pltpu.make_async_copy(
            values_hbm.at[pl.ds(p * 2, 2)], values.at[pl.ds(p * 2, 2)], value_sems.at[p]
        )
        for p in range(pairs)
    ]
    out_copy = pltpu.make_async_copy(out_hbm, out_w, out_sem)
    for copy in small:
        copy.start()
    for copy in first:
        copy.start()
    for copy in reversed(key_copies):
        copy.start()
    for copy in value_copies:
        copy.start()
    out_copy.start()

    for copy in small:
        copy.wait()
    hidden_f = hidden[...].astype(f32)
    normed = rms_rows(hidden_f, attn_gain[...])

    lane = iota((1, lanes), 1)
    lane_len = jnp.zeros((1, lanes), jnp.int32)
    for n in range(seqs):
        lane_len = jnp.where(lane // HEADS == n, lengths[n], lane_len)
    lane_bias = jnp.zeros((1, lanes), f32)
    for h in range(HEADS):
        lane_bias = jnp.where(lane % HEADS == h, score_bias[h], lane_bias)

    spread = (iota((lanes, seqs), 0) // HEADS == iota((lanes, seqs), 1)).astype(bf16)
    gather = (iota((seqs, lanes), 1) // HEADS == iota((seqs, lanes), 0)).astype(bf16)
    wide = (lanes, HEADS * HEAD)
    own_head = iota(wide, 1) // HEAD == iota(wide, 0) % HEADS
    fold_shape = (HEADS * HEAD, KV_WIDTH)
    fold = (
        (iota(fold_shape, 0) // (HEAD * GROUP) == iota(fold_shape, 1) // HEAD)
        & (iota(fold_shape, 0) % HEAD == iota(fold_shape, 1) % HEAD)
    ).astype(bf16)
    later = (iota((CHUNK, CHUNK), 1) > iota((CHUNK, CHUNK), 0)).astype(bf16)

    for copy in first:
        copy.wait()
    queries = matmul(normed, query_w[...]).astype(bf16)
    new_keys[...] = matmul(normed, key_w[...]).astype(bf16)
    new_values[...] = matmul(normed, value_w[...]).astype(bf16)

    spread_q = jnp.where(own_head, matmul(spread, queries), 0.0).astype(bf16)
    by_head = jnp.transpose(matmul(spread_q, fold))
    square = (KV_WIDTH, lanes)
    for n in range(seqs):
        own_lane = iota(square, 1) // HEADS == n
        blocked[n * KV_WIDTH : (n + 1) * KV_WIDTH, :] = jnp.where(own_lane, by_head, 0.0).astype(
            bf16
        )

    carry = jnp.zeros((1, lanes), f32)
    for c in reversed(range(chunks)):
        key_copies[c].wait()
        rows = slice(c * CHUNK, (c + 1) * CHUNK)
        key_rows = jnp.concatenate([keys[n, rows, :] for n in range(seqs)], axis=1)
        scores = matmul(key_rows, blocked[...]) * HEAD ** (-0.5) + lane_bias
        live = iota((CHUNK, lanes), 0) + c * CHUNK < lane_len
        soft = jnp.log1p(jnp.exp(-jnp.abs(scores)))
        log_keep = jnp.where(live, jnp.minimum(-scores, 0.0) - soft, 0.0)
        log_take = jnp.minimum(scores, 0.0) - soft
        sums = matmul(later, jnp.concatenate(three_parts(log_keep), axis=1))
        after = sums[:, :lanes] + sums[:, lanes : 2 * lanes] + sums[:, 2 * lanes :] + carry
        carry = carry + jnp.sum(log_keep, axis=0, keepdims=True)
        taken = jnp.where(live, jnp.exp(log_take + after), 0.0)
        weights_t[:, rows] = jnp.transpose(taken).astype(bf16)

    expert_copy.start()
    pieces = []
    for p in range(pairs):
        value_copies[p].wait()
        value_rows = jnp.concatenate([values[2 * p], values[2 * p + 1]], axis=1)
        mixed = matmul(weights_t[2 * p * HEADS : 2 * (p + 1) * HEADS, :], value_rows)
        pieces.append(mixed[:HEADS, :KV_WIDTH])
        pieces.append(mixed[HEADS:, KV_WIDTH:])
    mixed = jnp.concatenate(pieces, axis=0)
    own_group = (iota(mixed.shape, 0) % HEADS) // GROUP == iota(mixed.shape, 1) // HEAD
    mixed = jnp.where(own_group, mixed, 0.0).astype(bf16)
    unfolded = jnp.where(own_head, matmul_bt(mixed, fold), 0.0).astype(bf16)
    attended = matmul(gather, unfolded).astype(bf16)

    out_copy.wait()
    middle_f = hidden_f + matmul(attended, out_w[...])
    middle[...] = middle_f
    send_middle = pltpu.make_async_copy(middle, middle_hbm, send_sems.at[2])
    send_middle.start()
    ffn = rms_rows(middle_f, ffn_gain[...])
    ffn_in[...] = ffn
    send_ffn = pltpu.make_async_copy(ffn_in, ffn_hbm, send_sems.at[0])
    send_ffn.start()
    cut = outgoing.shape[1]
    stacked = jnp.concatenate(
        [ffn[:, j * cut : (j + 1) * cut] for j in range(ffn.shape[1] // cut)], axis=0
    )
    outgoing[...] = matmul(dispatch[...], stacked).astype(bf16)
    send_out = pltpu.make_async_copy(outgoing, outgoing_hbm, send_sems.at[1])
    send_out.start()
    gate_sum = jnp.sum(ffn.astype(f32) * branch_gate[...], axis=-1, keepdims=True)
    gate_value[...] = jnp.broadcast_to(jax.nn.sigmoid(gate_sum), gate_value.shape)
    expert_copy.wait()
    send_middle.wait()
    send_ffn.wait()
    send_out.wait()


SMEM = pl.BlockSpec(memory_space=pltpu.SMEM)
VMEM = pl.BlockSpec(memory_space=pltpu.VMEM)
HBM = pl.BlockSpec(memory_space=pltpu.HBM)


def in_hbm(values):
    return pltpu.with_memory_space_constraint(values, pltpu.HBM)


def call(kernel, out_shape, args, in_specs, out_specs, scratch=(), limit=16):
    return pl.pallas_call(
        kernel,
        out_shape=out_shape,
        in_specs=in_specs,
        out_specs=out_specs,
        scratch_shapes=list(scratch),
        compiler_params=pltpu.CompilerParams(vmem_limit_bytes=limit << 20),
    )(*args)


def shaped(shape, dtype):
    return jax.ShapeDtypeStruct(shape, dtype)


def attend(args, out_rows, out_cut):
    hidden = args[2]
    keys = args[10]
    seqs, width = hidden.shape
    cache_len = keys.shape[1]
    return call(
        attend_kernel,
        (
            shaped((seqs, KV_WIDTH), bf16),
            shaped((seqs, KV_WIDTH), bf16),
            pltpu.HBM((seqs, width), f32),
            pltpu.HBM((seqs, width), bf16),
            pltpu.HBM((out_rows, out_cut), bf16),
            shaped((seqs, 128), f32),
        )
        + tuple(pltpu.VMEM(a.shape, a.dtype) for a in args[13:]),
        tuple(arg if i == 6 else in_hbm(arg) for i, arg in enumerate(args)),
        [HBM] * 6 + [VMEM] + [HBM] * 7,
        [VMEM] * 2 + [HBM] * 3 + [VMEM] * 2,
        [
            pltpu.SMEM(args[0].shape, jnp.int32),
            pltpu.SMEM(args[1].shape, f32),
        ]
        + [pltpu.VMEM(a.shape, a.dtype) for a in args[2:6]]
        + [pltpu.VMEM(a.shape, a.dtype) for a in args[7:13]]
        + [
            pltpu.VMEM((seqs, width), f32),
            pltpu.VMEM((seqs, width), bf16),
            pltpu.VMEM((out_rows, out_cut), bf16),
            pltpu.VMEM((seqs * KV_WIDTH, seqs * HEADS), bf16),
            pltpu.VMEM((seqs * HEADS, cache_len), bf16),
            pltpu.SemaphoreType.DMA((6,)),
            pltpu.SemaphoreType.DMA((3,)),
            pltpu.SemaphoreType.DMA((cache_len // CHUNK,)),
            pltpu.SemaphoreType.DMA((seqs // 2,)),
            pltpu.SemaphoreType.DMA,
            pltpu.SemaphoreType.DMA,
            pltpu.SemaphoreType.DMA((3,)),
        ],
        32,
    )


def prepare(gate_t, up_t, down_t, routes_t, route_weights_t, capacity, cuts, experts):
    units, width = gate_t.shape
    seqs = routes_t.shape[1]
    rows = experts * capacity * cuts
    lanes = cuts * seqs
    half = units // 2

    def kernel(
        gate,
        up,
        down,
        picks_hbm,
        pick_weights_hbm,
        low,
        high,
        dispatch,
        combine_hbm,
        combine,
        picks,
        pick_weights,
        sems,
    ):
        small = [
            pltpu.make_async_copy(picks_hbm, picks, sems.at[4]),
            pltpu.make_async_copy(pick_weights_hbm, pick_weights, sems.at[5]),
        ]
        for copy in small:
            copy.start()
        copies = [
            pltpu.make_async_copy(gate, low.at[pl.ds(0, units)], sems.at[0]),
            pltpu.make_async_copy(
                up.at[pl.ds(0, half)], low.at[pl.ds(units, half)], sems.at[1]
            ),
            pltpu.make_async_copy(
                up.at[pl.ds(half, half)], high.at[pl.ds(0, half)], sems.at[2]
            ),
            pltpu.make_async_copy(down, high.at[pl.ds(half, units)], sems.at[3]),
        ]
        for copy in copies:
            copy.start()
        for copy in small:
            copy.wait()
        shape = (rows, seqs)
        expert = iota(shape, 0) // (capacity * cuts)
        named = jnp.zeros(shape, f32)
        weighted = jnp.zeros(shape, f32)
        for k in range(TOP):
            hit = expert == picks[k : k + 1, :]
            named = named + jnp.where(hit, 1.0, 0.0)
            weighted = weighted + jnp.where(hit, pick_weights[k : k + 1, :], 0.0)
        earlier = (iota((seqs, seqs), 0) < iota((seqs, seqs), 1)).astype(bf16)
        rank = matmul(named.astype(bf16), earlier)
        mine = rank == (iota(shape, 0) % capacity).astype(f32)
        repeat = (iota((seqs, lanes), 1) % seqs == iota((seqs, lanes), 0)).astype(bf16)
        own_cut = (iota((rows, lanes), 0) // capacity) % cuts == iota((rows, lanes), 1) // seqs

        def spread(values):
            return jnp.where(own_cut, matmul(values, repeat), 0.0).astype(bf16)

        dispatch[...] = spread(jnp.where(mine, named, 0.0).astype(bf16))
        parts = three_parts(jnp.where(mine, weighted, 0.0))
        for part in range(3):
            combine[:, part * lanes : (part + 1) * lanes] = spread(parts[part])
        send = pltpu.make_async_copy(combine, combine_hbm, sems.at[6])
        send.start()
        send.wait()
        for copy in copies:
            copy.wait()

    return call(
        kernel,
        (
            shaped((units + half, width), bf16),
            shaped((units + half, width), bf16),
            shaped((rows, lanes), bf16),
            pltpu.HBM((rows, 3 * lanes), bf16),
        ),
        (gate_t, up_t, down_t, routes_t, route_weights_t),
        [HBM] * 5,
        [HBM] * 2 + [VMEM] + [HBM],
        [
            pltpu.VMEM((rows, 3 * lanes), bf16),
            pltpu.VMEM(routes_t.shape, jnp.int32),
            pltpu.VMEM(route_weights_t.shape, f32),
            pltpu.SemaphoreType.DMA((7,)),
        ],
        32,
    )


def run_experts(arrived, gate_w, up_w, down_w, capacity):
    devices, chunk, cut = arrived.shape
    cuts = chunk // capacity
    block = min(devices, 256 // chunk)
    block_rows = block * chunk
    block_slots = block * capacity

    def kernel(rows, gate, up_hbm, down_hbm, out, up, down, sems):
        up_copy = pltpu.make_async_copy(up_hbm, up, sems.at[0])
        down_copy = pltpu.make_async_copy(down_hbm, down, sems.at[1])
        up_copy.start()
        down_copy.start()
        square = (block_rows, block_rows)

        def target(index):
            slot = index % block_slots
            return (
                slot // capacity * chunk + index // block_slots * capacity + slot % capacity
            )

        to_cuts = (target(iota(square, 0)) == iota(square, 1)).astype(bf16)
        to_chunks = (target(iota(square, 1)) == iota(square, 0)).astype(bf16)
        tokens = []
        for b in range(devices // block):
            part = rows[b * block : (b + 1) * block].reshape(block_rows, cut)
            sorted_rows = matmul(to_cuts, part).astype(bf16)
            tokens.append(
                jnp.concatenate(
                    [
                        sorted_rows[j * block_slots : (j + 1) * block_slots]
                        for j in range(cuts)
                    ],
                    axis=1,
                )
            )
        tokens = jnp.concatenate(tokens, axis=0)
        hidden = jax.nn.silu(matmul(tokens, gate[...]))
        up_copy.wait()
        hidden = hidden * matmul(tokens, up[...])
        down_copy.wait()
        result = matmul(hidden.astype(bf16), down[...]).astype(bf16)
        for b in range(devices // block):
            part = result[b * block_slots : (b + 1) * block_slots]
            part = jnp.concatenate(
                [part[:, j * cut : (j + 1) * cut] for j in range(cuts)], axis=0
            )
            out[b * block : (b + 1) * block] = (
                matmul(to_chunks, part).astype(bf16).reshape(block, chunk, cut)
            )

    return call(
        kernel,
        shaped(arrived.shape, bf16),
        (arrived, gate_w, in_hbm(up_w), in_hbm(down_w)),
        [VMEM] * 2 + [HBM] * 2,
        VMEM,
        [
            pltpu.VMEM(up_w.shape, up_w.dtype),
            pltpu.VMEM(down_w.shape, down_w.dtype),
            pltpu.SemaphoreType.DMA((2,)),
        ],
        32,
    )


def run_dense(tokens, lows, highs):
    seqs, width = tokens[0].shape
    count = len(lows)
    held = lows[0].shape[0]
    half = held // 3
    units = 2 * half
    total = len(tokens)
    kept = total // 2 * seqs

    def kernel(*refs):
        token_refs = refs[:total]
        sources = refs[total : total + 2 * count]
        keep, give = refs[total + 2 * count : total + 2 * count + 2]
        weights, sems = refs[total + 2 * count + 2 :]
        copies = [
            pltpu.make_async_copy(source, weights.at[i], sems.at[i])
            for i, source in enumerate(sources)
        ]
        for copy in copies:
            copy.start()
        rows = jnp.concatenate([ref[...] for ref in token_refs], axis=0)
        for copy in copies:
            copy.wait()
        gates = [weights[j, :units] for j in range(count)]
        ups = []
        for j in range(count):
            ups += [weights[j, units:], weights[count + j, :half]]
        downs = [weights[count + j, half:] for j in range(count)]
        hidden = jax.nn.silu(matmul_bt(rows, jnp.concatenate(gates, axis=0)))
        hidden = hidden * matmul_bt(rows, jnp.concatenate(ups, axis=0))
        partial = matmul(hidden.astype(bf16), jnp.concatenate(downs, axis=0))
        keep[...] = partial[:kept]
        give[...] = partial[kept:].astype(bf16)

    return call(
        kernel,
        (shaped((kept, width), f32), shaped((total * seqs - kept, width), bf16)),
        (*tokens, *lows, *highs),
        [VMEM] * total + [HBM] * (2 * count),
        [VMEM] * 2,
        [pltpu.VMEM((2 * count, held, width), bf16), pltpu.SemaphoreType.DMA((2 * count,))],
        32,
    )


def merge(kept, taken, seqs):
    layers = kept.shape[0] // seqs
    width = kept.shape[1]

    def kernel(left, right, own, *rest):
        own[...] = left[:seqs] + right[:seqs].astype(f32)
        for k in range(1, layers):
            rows = slice(k * seqs, (k + 1) * seqs)
            rest[k - 1][...] = (left[rows] + right[rows].astype(f32)).astype(bf16)

    return call(
        kernel,
        (shaped((seqs, width), f32),) + (shaped((seqs, width), bf16),) * (layers - 1),
        (kept, taken),
        [VMEM] * 2,
        [VMEM] * layers,
    )


def finish(middle, gate_value, combine, returned, dense_parts):
    seqs, width = middle.shape
    devices, chunk, cut = returned.shape
    lanes = combine.shape[1] // 3

    def kernel(base, gate, mix, rows, *refs):
        out = refs[-1]
        picked = rows[...].reshape(devices * chunk, cut)
        mixed = matmul_at(mix[...], picked)
        mixed = mixed[:lanes] + mixed[lanes : 2 * lanes] + mixed[2 * lanes :]
        dense = refs[0][...]
        for ref in refs[1:-1]:
            dense = dense + ref[...].astype(f32)
        expert_sum = jnp.concatenate(
            [mixed[j * seqs : (j + 1) * seqs] for j in range(width // cut)], axis=1
        )
        out[...] = (base[...] + expert_sum + gate[:, :1] * dense).astype(bf16)

    return call(
        kernel,
        shaped((seqs, width), bf16),
        (middle, gate_value, combine, returned, *dense_parts),
        [VMEM] * (4 + len(dense_parts)),
        VMEM,
        (),
        32,
    )


def per_device(
    hidden_in,
    lengths,
    attn_gain,
    query_weight,
    key_weight,
    value_weight,
    score_bias,
    out_weight,
    key_cache,
    value_cache,
    ffn_gain,
    routes,
    route_weights,
    expert_gate,
    expert_up,
    expert_down,
    dense_gate,
    dense_up,
    dense_down,
    branch_gate,
):
    seqs, width = hidden_in.shape
    devices = lax.axis_size("ep")
    experts_all = expert_gate.shape[0] * devices
    capacity = max(1, seqs * TOP // experts_all)
    cuts = max(1, 16 // capacity)
    chunk = capacity * cuts
    layers = layer_count(devices)
    plane = devices // layers

    def swap(values, bits):
        return lax.ppermute(values, "ep", [(i, i ^ bits) for i in range(devices)])

    def climb(values, steps):
        return lax.ppermute(
            values, "ep", [(i, (i + steps * plane) % devices) for i in range(devices)]
        )

    low, high, dispatch, combine = prepare(
        in_hbm(dense_gate.T),
        in_hbm(dense_up.T),
        in_hbm(dense_down.T),
        in_hbm(routes.T),
        in_hbm(route_weights.T),
        capacity,
        cuts,
        experts_all,
    )
    lows = [low]
    highs = [high]
    bits = 2
    while bits < plane:
        more_lows = [swap(low, bits)]
        more_highs = [swap(high, bits)]
        bits = 2 * bits
        lows += more_lows
        highs += more_highs
    bits = 2
    direct = {1 << (k + 1): k + 1 for k in range(len(lows) - 1)}
    for other in range(2, plane, 2):
        if other in direct:
            continue
        first = other & -other
        last = other ^ first
        if last in direct:
            lows.append(swap(lows[direct[first]], last))
            highs.append(swap(highs[direct[last]], first))
        else:
            lows.append(swap(low, other))
            highs.append(swap(high, other))

    new_keys, new_values, middle, ffn_in, outgoing, gate_value, gate_w = attend(
        (
            lengths,
            score_bias,
            hidden_in,
            attn_gain.reshape(1, width),
            ffn_gain.reshape(1, width),
            branch_gate.reshape(1, width),
            dispatch,
            query_weight,
            key_weight,
            value_weight,
            key_cache,
            value_cache,
            out_weight,
            expert_gate[0],
        ),
        devices * chunk,
        width // cuts,
    )
    arrived = lax.all_to_all(
        outgoing.reshape(devices, chunk, width // cuts),
        "ep",
        split_axis=0,
        concat_axis=0,
        tiled=True,
    )
    chain = [ffn_in]
    for k in range(1, layers):
        chain.append(climb(ffn_in, k))
    for k in range(layers):
        chain.append(swap(chain[k], 1))
    expert_rows = run_experts(arrived, gate_w, expert_up[0], expert_down[0], capacity)
    returned = lax.all_to_all(
        expert_rows, "ep", split_axis=0, concat_axis=0, tiled=True
    )
    kept, given = run_dense(chain, lows, highs)
    taken = swap(given, 1)
    own, *rest = merge(kept, taken, seqs)
    parts = [own]
    for k in range(1, layers):
        parts.append(climb(rest[k - 1], -k))
    hidden_out = finish(middle, gate_value, combine, returned, parts)
    return (hidden_out, new_keys, new_values)


def layer_count(devices):
    layers = 1
    while 2 * (2 * layers) ** 2 <= devices and devices % (4 * layers) == 0:
        layers = 2 * layers
    return layers


def solution(mesh):
    return jax.shard_map(
        per_device,
        mesh=mesh,
        in_specs=(
            P("ep", None),
            P("ep"),
            P(),
            P(),
            P(),
            P(),
            P(),
            P(),
            P("ep", None, None),
            P("ep", None, None),
            P(),
            P("ep", None),
            P("ep", None),
            P("ep", None, None),
            P("ep", None, None),
            P("ep", None, None),
            P(None, "ep"),
            P(None, "ep"),
            P(None, "ep"),
            P(),
        ),
        out_specs=(P("ep", None), P("ep", None), P("ep", None)),
        check_vma=False,
    )
```

```python
import jax
import jax.numpy as jnp
from jax import lax
from jax.experimental import pallas as pl
from jax.experimental.pallas import tpu as pltpu
from jax.sharding import PartitionSpec as P

HEADS = 8
KV_HEADS = 2
HEAD = 64
TOP = 4
GROUP = HEADS // KV_HEADS
KV_WIDTH = KV_HEADS * HEAD
CHUNK = 256


norm_eps = 1e-06
bf16 = jnp.bfloat16
f32 = jnp.float32


def iota(shape, dim):
    return lax.broadcasted_iota(jnp.int32, shape, dim)


def matmul(left, right):
    return jnp.dot(left, right, preferred_element_type=f32)


def matmul_bt(left, right):
    return lax.dot_general(left, right, (((1,), (1,)), ((), ())), preferred_element_type=f32)


def matmul_at(left, right):
    return lax.dot_general(left, right, (((0,), (0,)), ((), ())), preferred_element_type=f32)


def rms_rows(values, gain):
    scale = lax.rsqrt(jnp.mean(values * values, axis=-1, keepdims=True) + norm_eps)
    return (values * scale * gain).astype(bf16)


def three_parts(values):
    high = values.astype(bf16)
    rest = values - high.astype(f32)
    middle = rest.astype(bf16)
    low = (rest - middle.astype(f32)).astype(bf16)
    return high, middle, low


def attend_kernel(
    lengths_hbm,
    bias_hbm,
    hidden_hbm,
    attn_gain_hbm,
    ffn_gain_hbm,
    branch_hbm,
    dispatch,
    query_hbm,
    keys_hbm,
    values_hbm,
    out_hbm,
    expert_gate_hbm,
    middle_hbm,
    ffn_hbm,
    outgoing_hbm,
    gate_value,
    expert_gate,
    lengths,
    score_bias,
    hidden,
    attn_gain,
    ffn_gain,
    branch_gate,
    query_w,
    keys,
    values,
    out_w,
    middle,
    ffn_in,
    outgoing,
    blocked,
    weights_t,
    small_sems,
    query_sem,
    key_sems,
    value_sems,
    out_sem,
    expert_sem,
    send_sems,
):
    seqs = hidden.shape[0]
    cache_len = keys.shape[1]
    lanes = seqs * HEADS
    chunks = cache_len // CHUNK
    pairs = seqs // 2

    small = [
        pltpu.make_async_copy(source, target, small_sems.at[i])
        for i, (source, target) in enumerate(
            (
                (hidden_hbm, hidden),
                (attn_gain_hbm, attn_gain),
                (lengths_hbm, lengths),
                (bias_hbm, score_bias),
                (ffn_gain_hbm, ffn_gain),
                (branch_hbm, branch_gate),
            )
        )
    ]
    expert_copy = pltpu.make_async_copy(expert_gate_hbm, expert_gate, expert_sem)
    query_copy = pltpu.make_async_copy(query_hbm, query_w, query_sem)
    batches = key_sems.shape[0]
    batch = seqs // batches
    key_copies = [
        pltpu.make_async_copy(
            keys_hbm.at[pl.ds(b * batch, batch)], keys.at[pl.ds(b * batch, batch)], key_sems.at[b]
        )
        for b in range(batches)
    ]
    value_copies = [
        pltpu.make_async_copy(
            values_hbm.at[pl.ds(b * batch, batch)],
            values.at[pl.ds(b * batch, batch)],
            value_sems.at[b],
        )
        for b in range(batches)
    ]
    out_copy = pltpu.make_async_copy(out_hbm, out_w, out_sem)
    for copy in small:
        copy.start()
    query_copy.start()
    for copy in key_copies:
        copy.start()

    for copy in small:
        copy.wait()
    hidden_f = hidden[...].astype(f32)
    normed = rms_rows(hidden_f, attn_gain[...])

    lane = iota((1, lanes), 1)
    lane_len = jnp.zeros((1, lanes), jnp.int32)
    for n in range(seqs):
        lane_len = jnp.where(lane // HEADS == n, lengths[n], lane_len)
    lane_bias = jnp.zeros((1, lanes), f32)
    for h in range(HEADS):
        lane_bias = jnp.where(lane % HEADS == h, score_bias[h], lane_bias)

    spread = (iota((lanes, seqs), 0) // HEADS == iota((lanes, seqs), 1)).astype(bf16)
    gather = (iota((seqs, lanes), 1) // HEADS == iota((seqs, lanes), 0)).astype(bf16)
    wide = (lanes, HEADS * HEAD)
    own_head = iota(wide, 1) // HEAD == iota(wide, 0) % HEADS
    fold_shape = (HEADS * HEAD, KV_WIDTH)
    fold = (
        (iota(fold_shape, 0) // (HEAD * GROUP) == iota(fold_shape, 1) // HEAD)
        & (iota(fold_shape, 0) % HEAD == iota(fold_shape, 1) % HEAD)
    ).astype(bf16)
    later = (iota((CHUNK, CHUNK), 1) > iota((CHUNK, CHUNK), 0)).astype(bf16)

    query_copy.wait()
    for copy in value_copies:
        copy.start()
    out_copy.start()
    expert_copy.start()
    queries = matmul(normed, query_w[...]).astype(bf16)

    spread_q = jnp.where(own_head, matmul(spread, queries), 0.0).astype(bf16)
    by_head = jnp.transpose(matmul(spread_q, fold))
    square = (KV_WIDTH, lanes)
    for n in range(seqs):
        own_lane = iota(square, 1) // HEADS == n
        blocked[n * KV_WIDTH : (n + 1) * KV_WIDTH, :] = jnp.where(own_lane, by_head, 0.0).astype(
            bf16
        )

    for copy in key_copies:
        copy.wait()
    carry = jnp.zeros((1, lanes), f32)
    for c in reversed(range(chunks)):
        rows = slice(c * CHUNK, (c + 1) * CHUNK)
        key_rows = jnp.concatenate([keys[n, rows, :] for n in range(seqs)], axis=1)
        scores = matmul(key_rows, blocked[...]) * HEAD ** (-0.5) + lane_bias
        live = iota((CHUNK, lanes), 0) + c * CHUNK < lane_len
        soft = jnp.log1p(jnp.exp(-jnp.abs(scores)))
        log_keep = jnp.where(live, jnp.minimum(-scores, 0.0) - soft, 0.0)
        log_take = jnp.minimum(scores, 0.0) - soft
        sums = matmul(later, jnp.concatenate(three_parts(log_keep), axis=1))
        after = sums[:, :lanes] + sums[:, lanes : 2 * lanes] + sums[:, 2 * lanes :] + carry
        carry = carry + jnp.sum(log_keep, axis=0, keepdims=True)
        taken = jnp.where(live, jnp.exp(log_take + after), 0.0)
        weights_t[:, rows] = jnp.transpose(taken).astype(bf16)

    pieces = []
    for p in range(pairs):
        if 2 * p % batch == 0:
            value_copies[2 * p // batch].wait()
        value_rows = jnp.concatenate([values[2 * p], values[2 * p + 1]], axis=1)
        mixed = matmul(weights_t[2 * p * HEADS : 2 * (p + 1) * HEADS, :], value_rows)
        pieces.append(mixed[:HEADS, :KV_WIDTH])
        pieces.append(mixed[HEADS:, KV_WIDTH:])
    mixed = jnp.concatenate(pieces, axis=0)
    own_group = (iota(mixed.shape, 0) % HEADS) // GROUP == iota(mixed.shape, 1) // HEAD
    mixed = jnp.where(own_group, mixed, 0.0).astype(bf16)
    unfolded = jnp.where(own_head, matmul_bt(mixed, fold), 0.0).astype(bf16)
    attended = matmul(gather, unfolded).astype(bf16)

    out_copy.wait()
    middle_f = hidden_f + matmul(attended, out_w[...])
    middle[...] = middle_f
    send_middle = pltpu.make_async_copy(middle, middle_hbm, send_sems.at[2])
    send_middle.start()
    ffn = rms_rows(middle_f, ffn_gain[...])
    ffn_in[...] = ffn
    send_ffn = pltpu.make_async_copy(ffn_in, ffn_hbm, send_sems.at[0])
    send_ffn.start()
    cut = outgoing.shape[1]
    stacked = jnp.concatenate(
        [ffn[:, j * cut : (j + 1) * cut] for j in range(ffn.shape[1] // cut)], axis=0
    )
    outgoing[...] = matmul(dispatch[...], stacked).astype(bf16)
    send_out = pltpu.make_async_copy(outgoing, outgoing_hbm, send_sems.at[1])
    send_out.start()
    gate_sum = jnp.sum(ffn.astype(f32) * branch_gate[...], axis=-1, keepdims=True)
    gate_value[...] = jnp.broadcast_to(jax.nn.sigmoid(gate_sum), gate_value.shape)
    expert_copy.wait()
    send_middle.wait()
    send_ffn.wait()
    send_out.wait()


SMEM = pl.BlockSpec(memory_space=pltpu.SMEM)
VMEM = pl.BlockSpec(memory_space=pltpu.VMEM)
HBM = pl.BlockSpec(memory_space=pltpu.HBM)


def in_hbm(values):
    return pltpu.with_memory_space_constraint(values, pltpu.HBM)


def call(kernel, out_shape, args, in_specs, out_specs, scratch=(), limit=16):
    return pl.pallas_call(
        kernel,
        out_shape=out_shape,
        in_specs=in_specs,
        out_specs=out_specs,
        scratch_shapes=list(scratch),
        compiler_params=pltpu.CompilerParams(vmem_limit_bytes=limit << 20),
    )(*args)


def shaped(shape, dtype):
    return jax.ShapeDtypeStruct(shape, dtype)


def attend(args, out_rows, out_cut):
    hidden = args[2]
    keys = args[8]
    seqs, width = hidden.shape
    cache_len = keys.shape[1]
    return call(
        attend_kernel,
        (
            pltpu.HBM((seqs, width), f32),
            pltpu.HBM((seqs, width), bf16),
            pltpu.HBM((out_rows, out_cut), bf16),
            shaped((seqs, 128), f32),
        )
        + tuple(pltpu.VMEM(a.shape, a.dtype) for a in args[11:]),
        tuple(arg if i == 6 else in_hbm(arg) for i, arg in enumerate(args)),
        [HBM] * 6 + [VMEM] + [HBM] * 5,
        [HBM] * 3 + [VMEM] * 2,
        [
            pltpu.SMEM(args[0].shape, jnp.int32),
            pltpu.SMEM(args[1].shape, f32),
        ]
        + [pltpu.VMEM(a.shape, a.dtype) for a in args[2:6]]
        + [pltpu.VMEM(a.shape, a.dtype) for a in args[7:11]]
        + [
            pltpu.VMEM((seqs, width), f32),
            pltpu.VMEM((seqs, width), bf16),
            pltpu.VMEM((out_rows, out_cut), bf16),
            pltpu.VMEM((seqs * KV_WIDTH, seqs * HEADS), bf16),
            pltpu.VMEM((seqs * HEADS, cache_len), bf16),
            pltpu.SemaphoreType.DMA((6,)),
            pltpu.SemaphoreType.DMA,
            pltpu.SemaphoreType.DMA((4,)),
            pltpu.SemaphoreType.DMA((4,)),
            pltpu.SemaphoreType.DMA,
            pltpu.SemaphoreType.DMA,
            pltpu.SemaphoreType.DMA((3,)),
        ],
        32,
    )


def project(hidden, gain, key_w, value_w):
    def kernel(rows, gains, left, right, left_out, right_out):
        normed = rms_rows(rows[...].astype(f32), gains[...])
        left_out[...] = matmul(normed, left[...]).astype(bf16)
        right_out[...] = matmul(normed, right[...]).astype(bf16)

    return call(
        kernel,
        (shaped((hidden.shape[0], KV_WIDTH), bf16),) * 2,
        (hidden, gain, key_w, value_w),
        [VMEM] * 4,
        [VMEM] * 2,
    )


def prepare(gate_t, up_t, down_t, routes_t, route_weights_t, capacity, cuts, experts):
    units, width = gate_t.shape
    seqs = routes_t.shape[1]
    rows = experts * capacity * cuts
    lanes = cuts * seqs

    def kernel(
        gate,
        up,
        down,
        picks_hbm,
        pick_weights_hbm,
        own,
        dispatch,
        combine_hbm,
        combine,
        picks,
        pick_weights,
        sems,
    ):
        small = [
            pltpu.make_async_copy(picks_hbm, picks, sems.at[4]),
            pltpu.make_async_copy(pick_weights_hbm, pick_weights, sems.at[5]),
        ]
        for copy in small:
            copy.start()
        copies = [
            pltpu.make_async_copy(source, own.at[pl.ds(i * units, units)], sems.at[i])
            for i, source in enumerate((gate, up, down))
        ]
        for copy in copies:
            copy.start()
        for copy in small:
            copy.wait()
        shape = (rows, seqs)
        expert = iota(shape, 0) // (capacity * cuts)
        named = jnp.zeros(shape, f32)
        weighted = jnp.zeros(shape, f32)
        for k in range(TOP):
            hit = expert == picks[k : k + 1, :]
            named = named + jnp.where(hit, 1.0, 0.0)
            weighted = weighted + jnp.where(hit, pick_weights[k : k + 1, :], 0.0)
        earlier = (iota((seqs, seqs), 0) < iota((seqs, seqs), 1)).astype(bf16)
        rank = matmul(named.astype(bf16), earlier)
        mine = rank == (iota(shape, 0) % capacity).astype(f32)
        repeat = (iota((seqs, lanes), 1) % seqs == iota((seqs, lanes), 0)).astype(bf16)
        own_cut = (iota((rows, lanes), 0) // capacity) % cuts == iota((rows, lanes), 1) // seqs

        def spread(values):
            return jnp.where(own_cut, matmul(values, repeat), 0.0).astype(bf16)

        dispatch[...] = spread(jnp.where(mine, named, 0.0).astype(bf16))
        parts = three_parts(jnp.where(mine, weighted, 0.0))
        for part in range(3):
            combine[:, part * lanes : (part + 1) * lanes] = spread(parts[part])
        send = pltpu.make_async_copy(combine, combine_hbm, sems.at[6])
        send.start()
        send.wait()
        for copy in copies:
            copy.wait()

    return call(
        kernel,
        (
            shaped((3 * units, width), bf16),
            shaped((rows, lanes), bf16),
            pltpu.HBM((rows, 3 * lanes), bf16),
        ),
        (gate_t, up_t, down_t, routes_t, route_weights_t),
        [HBM] * 5,
        [HBM] + [VMEM] + [HBM],
        [
            pltpu.VMEM((rows, 3 * lanes), bf16),
            pltpu.VMEM(routes_t.shape, jnp.int32),
            pltpu.VMEM(route_weights_t.shape, f32),
            pltpu.SemaphoreType.DMA((7,)),
        ],
        32,
    )


def run_experts(arrived, gate_w, up_w, down_w, capacity):
    devices, chunk, cut = arrived.shape
    cuts = chunk // capacity
    block = min(devices, 256 // chunk)
    block_rows = block * chunk
    block_slots = block * capacity

    def kernel(rows, gate, up_hbm, down_hbm, out, up, down, sems):
        up_copy = pltpu.make_async_copy(up_hbm, up, sems.at[0])
        down_copy = pltpu.make_async_copy(down_hbm, down, sems.at[1])
        up_copy.start()
        down_copy.start()
        square = (block_rows, block_rows)

        def target(index):
            slot = index % block_slots
            return (
                slot // capacity * chunk + index // block_slots * capacity + slot % capacity
            )

        to_cuts = (target(iota(square, 0)) == iota(square, 1)).astype(bf16)
        to_chunks = (target(iota(square, 1)) == iota(square, 0)).astype(bf16)
        tokens = []
        for b in range(devices // block):
            part = rows[b * block : (b + 1) * block].reshape(block_rows, cut)
            sorted_rows = matmul(to_cuts, part).astype(bf16)
            tokens.append(
                jnp.concatenate(
                    [
                        sorted_rows[j * block_slots : (j + 1) * block_slots]
                        for j in range(cuts)
                    ],
                    axis=1,
                )
            )
        tokens = jnp.concatenate(tokens, axis=0)
        hidden = jax.nn.silu(matmul(tokens, gate[...]))
        up_copy.wait()
        hidden = hidden * matmul(tokens, up[...])
        down_copy.wait()
        result = matmul(hidden.astype(bf16), down[...]).astype(bf16)
        for b in range(devices // block):
            part = result[b * block_slots : (b + 1) * block_slots]
            part = jnp.concatenate(
                [part[:, j * cut : (j + 1) * cut] for j in range(cuts)], axis=0
            )
            out[b * block : (b + 1) * block] = (
                matmul(to_chunks, part).astype(bf16).reshape(block, chunk, cut)
            )

    return call(
        kernel,
        shaped(arrived.shape, bf16),
        (arrived, gate_w, in_hbm(up_w), in_hbm(down_w)),
        [VMEM] * 2 + [HBM] * 2,
        VMEM,
        [
            pltpu.VMEM(up_w.shape, up_w.dtype),
            pltpu.VMEM(down_w.shape, down_w.dtype),
            pltpu.SemaphoreType.DMA((2,)),
        ],
        32,
    )


def run_dense(tokens, pieces):
    seqs, width = tokens[0].shape
    count = len(pieces)
    units = pieces[0].shape[0] // 3
    total = len(tokens)
    kept = total // 2 * seqs

    def kernel(*refs):
        token_refs = refs[:total]
        sources = refs[total : total + count]
        keep, give, gates, ups, downs, sems = refs[total + count :]
        copies = [
            [
                pltpu.make_async_copy(
                    source.at[pl.ds(kind * units, units)],
                    target.at[pl.ds(i * units, units)],
                    sems.at[kind, i],
                )
                for i, source in enumerate(sources)
            ]
            for kind, target in enumerate((gates, ups, downs))
        ]
        for group in copies:
            for copy in group:
                copy.start()
        rows = jnp.concatenate([ref[...] for ref in token_refs], axis=0)
        for copy in copies[0]:
            copy.wait()
        hidden = jax.nn.silu(matmul_bt(rows, gates[...]))
        for copy in copies[1]:
            copy.wait()
        hidden = hidden * matmul_bt(rows, ups[...])
        for copy in copies[2]:
            copy.wait()
        partial = matmul(hidden.astype(bf16), downs[...])
        keep[...] = partial[:kept]
        give[...] = partial[kept:].astype(bf16)

    return call(
        kernel,
        (shaped((kept, width), f32), shaped((total * seqs - kept, width), bf16)),
        (*tokens, *pieces),
        [VMEM] * total + [HBM] * count,
        [VMEM] * 2,
        [pltpu.VMEM((count * units, width), bf16)] * 3 + [pltpu.SemaphoreType.DMA((3, count))],
        32,
    )


def merge(kept, taken, seqs):
    layers = kept.shape[0] // seqs
    width = kept.shape[1]

    def kernel(left, right, own, *rest):
        own[...] = left[:seqs] + right[:seqs].astype(f32)
        for k in range(1, layers):
            rows = slice(k * seqs, (k + 1) * seqs)
            rest[k - 1][...] = (left[rows] + right[rows].astype(f32)).astype(bf16)

    return call(
        kernel,
        (shaped((seqs, width), f32),) + (shaped((seqs, width), bf16),) * (layers - 1),
        (kept, taken),
        [VMEM] * 2,
        [VMEM] * layers,
    )


def finish(middle, gate_value, combine, returned, dense_parts):
    seqs, width = middle.shape
    devices, chunk, cut = returned.shape
    lanes = combine.shape[1] // 3

    def kernel(base, gate, mix, rows, *refs):
        out = refs[-1]
        picked = rows[...].reshape(devices * chunk, cut)
        mixed = matmul_at(mix[...], picked)
        mixed = mixed[:lanes] + mixed[lanes : 2 * lanes] + mixed[2 * lanes :]
        dense = refs[0][...]
        for ref in refs[1:-1]:
            dense = dense + ref[...].astype(f32)
        expert_sum = jnp.concatenate(
            [mixed[j * seqs : (j + 1) * seqs] for j in range(width // cut)], axis=1
        )
        out[...] = (base[...] + expert_sum + gate[:, :1] * dense).astype(bf16)

    return call(
        kernel,
        shaped((seqs, width), bf16),
        (middle, gate_value, combine, returned, *dense_parts),
        [VMEM] * (4 + len(dense_parts)),
        VMEM,
        (),
        32,
    )


def per_device(
    hidden_in,
    lengths,
    attn_gain,
    query_weight,
    key_weight,
    value_weight,
    score_bias,
    out_weight,
    key_cache,
    value_cache,
    ffn_gain,
    routes,
    route_weights,
    expert_gate,
    expert_up,
    expert_down,
    dense_gate,
    dense_up,
    dense_down,
    branch_gate,
):
    seqs, width = hidden_in.shape
    devices = lax.axis_size("ep")
    experts_all = expert_gate.shape[0] * devices
    capacity = max(1, seqs * TOP // experts_all)
    cuts = max(1, 16 // capacity)
    chunk = capacity * cuts
    layers = layer_count(devices)
    plane = devices // layers

    def swap(values, bits):
        return lax.ppermute(values, "ep", [(i, i ^ bits) for i in range(devices)])

    def climb(values, steps):
        return lax.ppermute(
            values, "ep", [(i, (i + steps * plane) % devices) for i in range(devices)]
        )

    own, dispatch, combine = prepare(
        in_hbm(dense_gate.T),
        in_hbm(dense_up.T),
        in_hbm(dense_down.T),
        in_hbm(routes.T),
        in_hbm(route_weights.T),
        capacity,
        cuts,
        experts_all,
    )
    pieces = [own]
    for other in range(2, plane, 2):
        pieces.append(swap(own, other))

    middle, ffn_in, outgoing, gate_value, gate_w = attend(
        (
            lengths,
            score_bias,
            hidden_in,
            attn_gain.reshape(1, width),
            ffn_gain.reshape(1, width),
            branch_gate.reshape(1, width),
            dispatch,
            query_weight,
            key_cache,
            value_cache,
            out_weight,
            expert_gate[0],
        ),
        devices * chunk,
        width // cuts,
    )
    arrived = lax.all_to_all(
        outgoing.reshape(devices, chunk, width // cuts),
        "ep",
        split_axis=0,
        concat_axis=0,
        tiled=True,
    )
    chain = [ffn_in]
    for k in range(1, layers):
        chain.append(climb(ffn_in, k))
    for k in range(layers):
        chain.append(swap(chain[k], 1))
    expert_rows = run_experts(arrived, gate_w, expert_up[0], expert_down[0], capacity)
    returned = lax.all_to_all(
        expert_rows, "ep", split_axis=0, concat_axis=0, tiled=True
    )
    kept, given = run_dense(chain, pieces)
    taken = swap(given, 1)
    own, *rest = merge(kept, taken, seqs)
    parts = [own]
    for k in range(1, layers):
        parts.append(climb(rest[k - 1], -k))
    new_keys, new_values = project(
        in_hbm(hidden_in),
        in_hbm(attn_gain.reshape(1, width)),
        in_hbm(key_weight),
        in_hbm(value_weight),
    )
    hidden_out = finish(middle, gate_value, combine, returned, parts)
    return (hidden_out, new_keys, new_values)


def layer_count(devices):
    layers = 1
    while 2 * (2 * layers) ** 2 <= devices and devices % (4 * layers) == 0:
        layers = 2 * layers
    return layers


def solution(mesh):
    return jax.shard_map(
        per_device,
        mesh=mesh,
        in_specs=(
            P("ep", None),
            P("ep"),
            P(),
            P(),
            P(),
            P(),
            P(),
            P(),
            P("ep", None, None),
            P("ep", None, None),
            P(),
            P("ep", None),
            P("ep", None),
            P("ep", None, None),
            P("ep", None, None),
            P("ep", None, None),
            P(None, "ep"),
            P(None, "ep"),
            P(None, "ep"),
            P(),
        ),
        out_specs=(P("ep", None), P("ep", None), P("ep", None)),
        check_vma=False,
    )
```

```python
import jax
import jax.numpy as jnp
from jax import lax
from jax.experimental import pallas as pl
from jax.experimental.pallas import tpu as pltpu
from jax.sharding import PartitionSpec as P

HEADS = 8
KV_HEADS = 2
HEAD = 64
TOP = 4
GROUP = HEADS // KV_HEADS
KV_WIDTH = KV_HEADS * HEAD
CHUNK = 256


norm_eps = 1e-06
bf16 = jnp.bfloat16
f32 = jnp.float32


def iota(shape, dim):
    return lax.broadcasted_iota(jnp.int32, shape, dim)


def matmul(left, right):
    return jnp.dot(left, right, preferred_element_type=f32)


def matmul_bt(left, right):
    return lax.dot_general(left, right, (((1,), (1,)), ((), ())), preferred_element_type=f32)


def matmul_at(left, right):
    return lax.dot_general(left, right, (((0,), (0,)), ((), ())), preferred_element_type=f32)


def rms_rows(values, gain):
    scale = lax.rsqrt(jnp.mean(values * values, axis=-1, keepdims=True) + norm_eps)
    return (values * scale * gain).astype(bf16)


def three_parts(values):
    high = values.astype(bf16)
    rest = values - high.astype(f32)
    middle = rest.astype(bf16)
    low = (rest - middle.astype(f32)).astype(bf16)
    return high, middle, low


def attend_kernel(
    capacity,
    lengths_hbm,
    bias_hbm,
    hidden_hbm,
    attn_gain_hbm,
    ffn_gain_hbm,
    branch_hbm,
    picks_hbm,
    pick_weights_hbm,
    query_hbm,
    keys_hbm,
    values_hbm,
    out_hbm,
    expert_gate_hbm,
    middle_hbm,
    ffn_hbm,
    outgoing_hbm,
    combine_hbm,
    gate_value,
    expert_gate,
    lengths,
    score_bias,
    hidden,
    attn_gain,
    ffn_gain,
    branch_gate,
    picks,
    pick_weights,
    query_w,
    keys,
    values,
    out_w,
    middle,
    ffn_in,
    outgoing,
    combine,
    dispatch,
    blocked,
    weights_t,
    small_sems,
    query_sem,
    key_sems,
    value_sems,
    out_sem,
    expert_sem,
    send_sems,
):
    seqs = hidden.shape[0]
    cache_len = keys.shape[1]
    lanes = seqs * HEADS
    chunks = cache_len // CHUNK
    pairs = seqs // 2

    small = [
        pltpu.make_async_copy(source, target, small_sems.at[i])
        for i, (source, target) in enumerate(
            (
                (hidden_hbm, hidden),
                (attn_gain_hbm, attn_gain),
                (lengths_hbm, lengths),
                (bias_hbm, score_bias),
                (ffn_gain_hbm, ffn_gain),
                (branch_hbm, branch_gate),
                (picks_hbm, picks),
                (pick_weights_hbm, pick_weights),
            )
        )
    ]
    expert_copy = pltpu.make_async_copy(expert_gate_hbm, expert_gate, expert_sem)
    query_copy = pltpu.make_async_copy(query_hbm, query_w, query_sem)
    batches = key_sems.shape[0]
    batch = seqs // batches
    key_copies = [
        pltpu.make_async_copy(
            keys_hbm.at[pl.ds(b * batch, batch)], keys.at[pl.ds(b * batch, batch)], key_sems.at[b]
        )
        for b in range(batches)
    ]
    value_copies = [
        pltpu.make_async_copy(
            values_hbm.at[pl.ds(b * batch, batch)],
            values.at[pl.ds(b * batch, batch)],
            value_sems.at[b],
        )
        for b in range(batches)
    ]
    out_copy = pltpu.make_async_copy(out_hbm, out_w, out_sem)
    for copy in small:
        copy.start()
    query_copy.start()
    for copy in key_copies:
        copy.start()

    for copy in small:
        copy.wait()
    hidden_f = hidden[...].astype(f32)
    normed = rms_rows(hidden_f, attn_gain[...])

    rows = outgoing.shape[0]
    cuts = hidden.shape[1] // outgoing.shape[1]
    shape = (rows, seqs)
    expert = iota(shape, 0) // (capacity * cuts)
    named = jnp.zeros(shape, f32)
    weighted = jnp.zeros(shape, f32)
    for k in range(TOP):
        hit = expert == picks[k : k + 1, :]
        named = named + jnp.where(hit, 1.0, 0.0)
        weighted = weighted + jnp.where(hit, pick_weights[k : k + 1, :], 0.0)
    earlier = (iota((seqs, seqs), 0) < iota((seqs, seqs), 1)).astype(bf16)
    rank = matmul(named.astype(bf16), earlier)
    mine = rank == (iota(shape, 0) % capacity).astype(f32)
    wide = (rows, cuts * seqs)
    repeat = (iota((seqs, wide[1]), 1) % seqs == iota((seqs, wide[1]), 0)).astype(bf16)
    own_cut = (iota(wide, 0) // capacity) % cuts == iota(wide, 1) // seqs

    def spread_cuts(values):
        return jnp.where(own_cut, matmul(values, repeat), 0.0).astype(bf16)

    dispatch[...] = spread_cuts(jnp.where(mine, named, 0.0).astype(bf16))
    parts = three_parts(jnp.where(mine, weighted, 0.0))
    for part in range(3):
        combine[:, part * wide[1] : (part + 1) * wide[1]] = spread_cuts(parts[part])
    send_combine = pltpu.make_async_copy(combine, combine_hbm, send_sems.at[3])
    send_combine.start()

    lane = iota((1, lanes), 1)
    lane_len = jnp.zeros((1, lanes), jnp.int32)
    for n in range(seqs):
        lane_len = jnp.where(lane // HEADS == n, lengths[n], lane_len)
    lane_bias = jnp.zeros((1, lanes), f32)
    for h in range(HEADS):
        lane_bias = jnp.where(lane % HEADS == h, score_bias[h], lane_bias)

    spread = (iota((lanes, seqs), 0) // HEADS == iota((lanes, seqs), 1)).astype(bf16)
    gather = (iota((seqs, lanes), 1) // HEADS == iota((seqs, lanes), 0)).astype(bf16)
    wide = (lanes, HEADS * HEAD)
    own_head = iota(wide, 1) // HEAD == iota(wide, 0) % HEADS
    fold_shape = (HEADS * HEAD, KV_WIDTH)
    fold = (
        (iota(fold_shape, 0) // (HEAD * GROUP) == iota(fold_shape, 1) // HEAD)
        & (iota(fold_shape, 0) % HEAD == iota(fold_shape, 1) % HEAD)
    ).astype(bf16)
    later = (iota((CHUNK, CHUNK), 1) > iota((CHUNK, CHUNK), 0)).astype(bf16)

    query_copy.wait()
    for copy in value_copies:
        copy.start()
    out_copy.start()
    expert_copy.start()
    queries = matmul(normed, query_w[...]).astype(bf16)

    spread_q = jnp.where(own_head, matmul(spread, queries), 0.0).astype(bf16)
    by_head = jnp.transpose(matmul(spread_q, fold))
    square = (KV_WIDTH, lanes)
    for n in range(seqs):
        own_lane = iota(square, 1) // HEADS == n
        blocked[n * KV_WIDTH : (n + 1) * KV_WIDTH, :] = jnp.where(own_lane, by_head, 0.0).astype(
            bf16
        )

    for copy in key_copies:
        copy.wait()
    carry = jnp.zeros((1, lanes), f32)
    for c in reversed(range(chunks)):
        rows = slice(c * CHUNK, (c + 1) * CHUNK)
        key_rows = jnp.concatenate([keys[n, rows, :] for n in range(seqs)], axis=1)
        scores = matmul(key_rows, blocked[...]) * HEAD ** (-0.5) + lane_bias
        live = iota((CHUNK, lanes), 0) + c * CHUNK < lane_len
        soft = jnp.log1p(jnp.exp(-jnp.abs(scores)))
        log_keep = jnp.where(live, jnp.minimum(-scores, 0.0) - soft, 0.0)
        log_take = jnp.minimum(scores, 0.0) - soft
        sums = matmul(later, jnp.concatenate(three_parts(log_keep), axis=1))
        after = sums[:, :lanes] + sums[:, lanes : 2 * lanes] + sums[:, 2 * lanes :] + carry
        carry = carry + jnp.sum(log_keep, axis=0, keepdims=True)
        taken = jnp.where(live, jnp.exp(log_take + after), 0.0)
        weights_t[:, rows] = jnp.transpose(taken).astype(bf16)

    pieces = []
    for p in range(pairs):
        if 2 * p % batch == 0:
            value_copies[2 * p // batch].wait()
        value_rows = jnp.concatenate([values[2 * p], values[2 * p + 1]], axis=1)
        mixed = matmul(weights_t[2 * p * HEADS : 2 * (p + 1) * HEADS, :], value_rows)
        pieces.append(mixed[:HEADS, :KV_WIDTH])
        pieces.append(mixed[HEADS:, KV_WIDTH:])
    mixed = jnp.concatenate(pieces, axis=0)
    own_group = (iota(mixed.shape, 0) % HEADS) // GROUP == iota(mixed.shape, 1) // HEAD
    mixed = jnp.where(own_group, mixed, 0.0).astype(bf16)
    unfolded = jnp.where(own_head, matmul_bt(mixed, fold), 0.0).astype(bf16)
    attended = matmul(gather, unfolded).astype(bf16)

    out_copy.wait()
    middle_f = hidden_f + matmul(attended, out_w[...])
    middle[...] = middle_f
    send_middle = pltpu.make_async_copy(middle, middle_hbm, send_sems.at[2])
    send_middle.start()
    ffn = rms_rows(middle_f, ffn_gain[...])
    ffn_in[...] = ffn
    send_ffn = pltpu.make_async_copy(ffn_in, ffn_hbm, send_sems.at[0])
    send_ffn.start()
    cut = outgoing.shape[1]
    stacked = jnp.concatenate(
        [ffn[:, j * cut : (j + 1) * cut] for j in range(ffn.shape[1] // cut)], axis=0
    )
    outgoing[...] = matmul(dispatch[...], stacked).astype(bf16)
    send_out = pltpu.make_async_copy(outgoing, outgoing_hbm, send_sems.at[1])
    send_out.start()
    gate_sum = jnp.sum(ffn.astype(f32) * branch_gate[...], axis=-1, keepdims=True)
    gate_value[...] = jnp.broadcast_to(jax.nn.sigmoid(gate_sum), gate_value.shape)
    expert_copy.wait()
    send_middle.wait()
    send_ffn.wait()
    send_out.wait()
    send_combine.wait()


SMEM = pl.BlockSpec(memory_space=pltpu.SMEM)
VMEM = pl.BlockSpec(memory_space=pltpu.VMEM)
HBM = pl.BlockSpec(memory_space=pltpu.HBM)


def in_hbm(values):
    return pltpu.with_memory_space_constraint(values, pltpu.HBM)


def call(kernel, out_shape, args, in_specs, out_specs, scratch=(), limit=16):
    return pl.pallas_call(
        kernel,
        out_shape=out_shape,
        in_specs=in_specs,
        out_specs=out_specs,
        scratch_shapes=list(scratch),
        compiler_params=pltpu.CompilerParams(vmem_limit_bytes=limit << 20),
    )(*args)


def shaped(shape, dtype):
    return jax.ShapeDtypeStruct(shape, dtype)


def attend(args, capacity, out_rows, out_cut):
    hidden = args[2]
    keys = args[9]
    seqs, width = hidden.shape
    cache_len = keys.shape[1]
    lanes = width // out_cut * seqs
    return call(
        lambda *refs: attend_kernel(capacity, *refs),
        (
            pltpu.HBM((seqs, width), f32),
            pltpu.HBM((seqs, width), bf16),
            pltpu.HBM((out_rows, out_cut), bf16),
            pltpu.HBM((out_rows, 3 * lanes), bf16),
            shaped((seqs, 128), f32),
            pltpu.VMEM(args[12].shape, bf16),
        ),
        tuple(in_hbm(arg) for arg in args),
        [HBM] * 13,
        [HBM] * 4 + [VMEM] * 2,
        [
            pltpu.SMEM(args[0].shape, jnp.int32),
            pltpu.SMEM(args[1].shape, f32),
        ]
        + [pltpu.VMEM(a.shape, a.dtype) for a in args[2:12]]
        + [
            pltpu.VMEM((seqs, width), f32),
            pltpu.VMEM((seqs, width), bf16),
            pltpu.VMEM((out_rows, out_cut), bf16),
            pltpu.VMEM((out_rows, 3 * lanes), bf16),
            pltpu.VMEM((out_rows, lanes), bf16),
            pltpu.VMEM((seqs * KV_WIDTH, seqs * HEADS), bf16),
            pltpu.VMEM((seqs * HEADS, cache_len), bf16),
            pltpu.SemaphoreType.DMA((8,)),
            pltpu.SemaphoreType.DMA,
            pltpu.SemaphoreType.DMA((4,)),
            pltpu.SemaphoreType.DMA((4,)),
            pltpu.SemaphoreType.DMA,
            pltpu.SemaphoreType.DMA,
            pltpu.SemaphoreType.DMA((4,)),
        ],
        40,
    )


def project(hidden, gain, key_w, value_w):
    def kernel(rows, gains, left, right, left_out, right_out):
        normed = rms_rows(rows[...].astype(f32), gains[...])
        left_out[...] = matmul(normed, left[...]).astype(bf16)
        right_out[...] = matmul(normed, right[...]).astype(bf16)

    return call(
        kernel,
        (shaped((hidden.shape[0], KV_WIDTH), bf16),) * 2,
        (hidden, gain, key_w, value_w),
        [VMEM] * 4,
        [VMEM] * 2,
    )


def run_experts(arrived, gate_w, up_w, down_w, capacity):
    devices, chunk, cut = arrived.shape
    cuts = chunk // capacity
    block = min(devices, 256 // chunk)
    block_rows = block * chunk
    block_slots = block * capacity

    def kernel(rows, gate, up_hbm, down_hbm, out, up, down, sems):
        up_copy = pltpu.make_async_copy(up_hbm, up, sems.at[0])
        down_copy = pltpu.make_async_copy(down_hbm, down, sems.at[1])
        up_copy.start()
        down_copy.start()
        square = (block_rows, block_rows)

        def target(index):
            slot = index % block_slots
            return (
                slot // capacity * chunk + index // block_slots * capacity + slot % capacity
            )

        to_cuts = (target(iota(square, 0)) == iota(square, 1)).astype(bf16)
        to_chunks = (target(iota(square, 1)) == iota(square, 0)).astype(bf16)
        tokens = []
        for b in range(devices // block):
            part = rows[b * block : (b + 1) * block].reshape(block_rows, cut)
            sorted_rows = matmul(to_cuts, part).astype(bf16)
            tokens.append(
                jnp.concatenate(
                    [
                        sorted_rows[j * block_slots : (j + 1) * block_slots]
                        for j in range(cuts)
                    ],
                    axis=1,
                )
            )
        tokens = jnp.concatenate(tokens, axis=0)
        hidden = jax.nn.silu(matmul(tokens, gate[...]))
        up_copy.wait()
        hidden = hidden * matmul(tokens, up[...])
        down_copy.wait()
        result = matmul(hidden.astype(bf16), down[...]).astype(bf16)
        for b in range(devices // block):
            part = result[b * block_slots : (b + 1) * block_slots]
            part = jnp.concatenate(
                [part[:, j * cut : (j + 1) * cut] for j in range(cuts)], axis=0
            )
            out[b * block : (b + 1) * block] = (
                matmul(to_chunks, part).astype(bf16).reshape(block, chunk, cut)
            )

    return call(
        kernel,
        shaped(arrived.shape, bf16),
        (arrived, gate_w, in_hbm(up_w), in_hbm(down_w)),
        [VMEM] * 2 + [HBM] * 2,
        VMEM,
        [
            pltpu.VMEM(up_w.shape, up_w.dtype),
            pltpu.VMEM(down_w.shape, down_w.dtype),
            pltpu.SemaphoreType.DMA((2,)),
        ],
        32,
    )


def run_dense(tokens, pieces):
    seqs, width = tokens[0].shape
    count = len(pieces) // 3
    units = pieces[0].shape[0]
    total = len(tokens)
    kept = total // 2 * seqs

    def kernel(*refs):
        token_refs = refs[:total]
        sources = refs[total : total + 3 * count]
        keep, give, weights, sems = refs[total + 3 * count :]
        copies = [
            pltpu.make_async_copy(
                source, weights.at[i // count, pl.ds(i % count * units, units)], sems.at[i]
            )
            for i, source in enumerate(sources)
        ]
        for copy in copies:
            copy.start()
        rows = jnp.concatenate([ref[...] for ref in token_refs], axis=0)
        for copy in copies[:count]:
            copy.wait()
        hidden = jax.nn.silu(matmul_bt(rows, weights[0]))
        for copy in copies[count : 2 * count]:
            copy.wait()
        hidden = hidden * matmul_bt(rows, weights[1])
        for copy in copies[2 * count :]:
            copy.wait()
        partial = matmul(hidden.astype(bf16), weights[2])
        keep[...] = partial[:kept]
        give[...] = partial[kept:].astype(bf16)

    return call(
        kernel,
        (shaped((kept, width), f32), shaped((total * seqs - kept, width), bf16)),
        (*tokens, *pieces),
        [VMEM] * total + [HBM] * (3 * count),
        [VMEM] * 2,
        [
            pltpu.VMEM((3, count * units, width), bf16),
            pltpu.SemaphoreType.DMA((3 * count,)),
        ],
        32,
    )


def merge(kept, taken, seqs):
    layers = kept.shape[0] // seqs
    width = kept.shape[1]

    def kernel(left, right, own, *rest):
        own[...] = left[:seqs] + right[:seqs].astype(f32)
        for k in range(1, layers):
            rows = slice(k * seqs, (k + 1) * seqs)
            rest[k - 1][...] = (left[rows] + right[rows].astype(f32)).astype(bf16)

    return call(
        kernel,
        (shaped((seqs, width), f32),) + (shaped((seqs, width), bf16),) * (layers - 1),
        (kept, taken),
        [VMEM] * 2,
        [VMEM] * layers,
    )


def finish(middle, gate_value, combine, returned, dense_parts):
    seqs, width = middle.shape
    devices, chunk, cut = returned.shape
    lanes = combine.shape[1] // 3

    def kernel(base, gate, mix, rows, *refs):
        out = refs[-1]
        picked = rows[...].reshape(devices * chunk, cut)
        mixed = matmul_at(mix[...], picked)
        mixed = mixed[:lanes] + mixed[lanes : 2 * lanes] + mixed[2 * lanes :]
        dense = refs[0][...]
        for ref in refs[1:-1]:
            dense = dense + ref[...].astype(f32)
        expert_sum = jnp.concatenate(
            [mixed[j * seqs : (j + 1) * seqs] for j in range(width // cut)], axis=1
        )
        out[...] = (base[...] + expert_sum + gate[:, :1] * dense).astype(bf16)

    return call(
        kernel,
        shaped((seqs, width), bf16),
        (middle, gate_value, combine, returned, *dense_parts),
        [VMEM] * (4 + len(dense_parts)),
        VMEM,
        (),
        32,
    )


def per_device(
    hidden_in,
    lengths,
    attn_gain,
    query_weight,
    key_weight,
    value_weight,
    score_bias,
    out_weight,
    key_cache,
    value_cache,
    ffn_gain,
    routes,
    route_weights,
    expert_gate,
    expert_up,
    expert_down,
    dense_gate,
    dense_up,
    dense_down,
    branch_gate,
):
    seqs, width = hidden_in.shape
    devices = lax.axis_size("ep")
    experts_all = expert_gate.shape[0] * devices
    capacity = max(1, seqs * TOP // experts_all)
    cuts = max(1, 16 // capacity)
    chunk = capacity * cuts
    layers = layer_count(devices)
    plane = devices // layers

    def swap(values, bits):
        return lax.ppermute(values, "ep", [(i, i ^ bits) for i in range(devices)])

    def climb(values, steps):
        return lax.ppermute(
            values, "ep", [(i, (i + steps * plane) % devices) for i in range(devices)]
        )

    own = {"gate": dense_gate.T, "up": dense_up.T, "down": dense_down.T}
    held = {0: own}
    for other in range(2, plane, 2):
        first, last = other & -other, other & (other - 1)
        held[other] = {}
        for kind, values in own.items():
            if last == 0 or last & (last - 1):
                held[other][kind] = swap(values, other)
            elif kind == "gate":
                held[other][kind] = swap(held[first][kind], last)
            else:
                held[other][kind] = swap(held[last][kind], first)
    pieces = [held[other][kind] for kind in own for other in held]

    middle, ffn_in, outgoing, combine, gate_value, gate_w = attend(
        (
            lengths,
            score_bias,
            hidden_in,
            attn_gain.reshape(1, width),
            ffn_gain.reshape(1, width),
            branch_gate.reshape(1, width),
            routes.T,
            route_weights.T,
            query_weight,
            key_cache,
            value_cache,
            out_weight,
            expert_gate[0],
        ),
        capacity,
        devices * chunk,
        width // cuts,
    )
    arrived = lax.all_to_all(
        outgoing.reshape(devices, chunk, width // cuts),
        "ep",
        split_axis=0,
        concat_axis=0,
        tiled=True,
    )
    chain = [ffn_in]
    for k in range(1, layers):
        chain.append(climb(ffn_in, k))
    for k in range(layers):
        chain.append(swap(chain[k], 1))
    expert_rows = run_experts(arrived, gate_w, expert_up[0], expert_down[0], capacity)
    returned = lax.all_to_all(
        expert_rows, "ep", split_axis=0, concat_axis=0, tiled=True
    )
    kept, given = run_dense(chain, pieces)
    taken = swap(given, 1)
    own, *rest = merge(kept, taken, seqs)
    parts = [own]
    for k in range(1, layers):
        parts.append(climb(rest[k - 1], -k))
    new_keys, new_values = project(
        in_hbm(hidden_in),
        in_hbm(attn_gain.reshape(1, width)),
        in_hbm(key_weight),
        in_hbm(value_weight),
    )
    hidden_out = finish(middle, gate_value, combine, returned, parts)
    return (hidden_out, new_keys, new_values)


def layer_count(devices):
    layers = 1
    while 2 * (2 * layers) ** 2 <= devices and devices % (4 * layers) == 0:
        layers = 2 * layers
    return layers


def solution(mesh):
    return jax.shard_map(
        per_device,
        mesh=mesh,
        in_specs=(
            P("ep", None),
            P("ep"),
            P(),
            P(),
            P(),
            P(),
            P(),
            P(),
            P("ep", None, None),
            P("ep", None, None),
            P(),
            P("ep", None),
            P("ep", None),
            P("ep", None, None),
            P("ep", None, None),
            P("ep", None, None),
            P(None, "ep"),
            P(None, "ep"),
            P(None, "ep"),
            P(),
        ),
        out_specs=(P("ep", None), P("ep", None), P("ep", None)),
        check_vma=False,
    )
```
